32 devices in a mesh: sp: 16 (over z, y, x), tp: 2 (over core).
Axes of the slice: x: 2, y: 2, z: 4, core: 2. Of those that a mesh axis runs over, the one named last changes fastest.
Arguments:
- tokens: bfloat16 [2048, 2048], P('sp'), may hold values from -6 to 6
- norm_gain: float32 [2048], replicated, may hold values from 0.1 to 1.9
- conv_value_weight: bfloat16 [2048, 1024], P('sp', 'tp'), may hold values from -0.125 to 0.125
- conv_gate_weight: bfloat16 [2048, 1024], P('sp', 'tp'), may hold values from -0.125 to 0.125
- conv_kernel: float32 [31, 1024], P(None, 'tp'), may hold values from -10 to 10
- conv_bias: float32 [1024], P('tp'), may hold values from -4 to 4
- channel_gain: float32 [1024], P('tp'), may hold values from 0.1 to 1.9
- query_weight: bfloat16 [2048, 2048], P('sp', 'tp'), may hold values from -0.125 to 0.125
- key_weight: bfloat16 [2048, 2048], P('sp', 'tp'), may hold values from -0.125 to 0.125
- value_weight: bfloat16 [2048, 4096], P('sp', 'tp'), may hold values from -0.125 to 0.125
- gate_weight: bfloat16 [2048, 32], replicated, may hold values from -0.125 to 0.125
- gate_offset: float32 [2, 2, 8, 2048], P(None, None, 'tp', 'sp'), may hold values from -110 to 160, as said below
- start_memory: float32 [2, 8, 512, 256], P(None, 'tp'), may hold values from -0.375 to 0.375
- start_norm: float32 [2, 8, 256], P(None, 'tp'), may hold values from -0.375 to 0.375
- start_level: float32 [2, 8], P(None, 'tp'), may hold values from 2 to 5
- cell_gain: float32 [4096], P('tp'), may hold values from 0.1 to 1.9
- out_conv_weight: bfloat16 [2048, 1024], P('sp', 'tp'), may hold values from -0.25 to 0.25
- out_cell_weight: bfloat16 [2048, 4096], P('sp', 'tp'), may hold values from -0.09375 to 0.09375
Outputs:
- mixed: bfloat16 [2048, 2048], P(('sp', 'tp'))
The draws below stay inside these ranges and needn't reach their ends.
Inputs may be any that keep to these rules, and one draw needn't show every extreme that they name: `gate_offset`: added to the gate pre-activations; index 0 of the second dimension is the input gate, index 1 the forget gate.
All inputs are finite; a program needn't handle non-finite values.
Results may differ from the reference program's by a relative error of at most 0.017.
Values may be sent and summed in bfloat16 or wider, within the bound.
No kernel may reach another device: no remote copies, remote signals or barrier semaphores. Data moves between devices by JAX's collectives and lax.ppermute only.
A program may use at most 192 MiB of HBM per device.

```python
import math
import jax
import jax.numpy as jnp
from jax import lax

D = 2048
CONV_W = 1024
MEMORY_GROUPS = 8
KEY_DIM = 256
VALUE_DIM = 512
KERNEL = 31
BLOCK = 128
TOK_DEV = 128
STEP_COUNT = 2048
N_TP = 2


def draw_conv_kernel(key, part):
    base_key, rough_key = jax.random.split(jax.random.fold_in(key, 11))
    channel = jnp.arange(CONV_W, dtype=jnp.float32) / CONV_W
    roughness = jnp.exp(jax.random.uniform(rough_key, (CONV_W,), minval=-0.5, maxval=0.5))
    channel_scale = jnp.exp(math.log(8.0) * channel)
    entries = jnp.clip(jax.random.normal(base_key, (KERNEL, CONV_W)), -4.0, 4.0)
    return (entries * channel_scale * roughness / math.sqrt(KERNEL)).astype(jnp.float32)


def draw_gate_offset(key, part):
    frequency_seed, permute_seed, surge_seed, feature_seed = jax.random.split(jax.random.fold_in(key, 23), 4)
    step_index = jnp.arange(STEP_COUNT)
    device_block = step_index // TOK_DEV
    device_count = STEP_COUNT // TOK_DEV
    device_rate = jnp.exp(jax.random.uniform(frequency_seed, (2, MEMORY_GROUPS, device_count), minval=math.log(0.4), maxval=math.log(2.5)))
    rate_here = jnp.take(device_rate, device_block, axis=2)
    order_keys = jax.random.split(permute_seed, 2)
    head_rank = jnp.stack([jax.random.permutation(order_keys[0], MEMORY_GROUPS), jax.random.permutation(order_keys[1], MEMORY_GROUPS)])
    fast_count = MEMORY_GROUPS // 2
    slow_level = jnp.log(2.0 * STEP_COUNT / rate_here)
    input_part = jnp.clip(jax.random.normal(feature_seed, (2, MEMORY_GROUPS, STEP_COUNT)), -4.0, 4.0)
    fast_head = (head_rank < fast_count)[:, :, None]
    surge_index = jax.random.randint(surge_seed, (2, MEMORY_GROUPS, 2), 0, STEP_COUNT)
    surge_flags = jnp.any(step_index[None, None, None, :] == surge_index[:, :, :, None], axis=2)
    decay_fraction = jnp.where(fast_head, 3.2, slow_level)
    decay_fraction = jnp.where(surge_flags, 0.5, decay_fraction)
    return jnp.stack([input_part, decay_fraction], axis=1).astype(jnp.float32)


def steps_of(stream_key, dims, pieces, smallest, largest):
    def one(dim, shards_of):
        heights = jax.random.uniform(jax.random.fold_in(jax.random.fold_in(stream_key, 6), dim), (shards_of,), jnp.float32, smallest / len(pieces), largest / len(pieces))
        return jnp.repeat(jnp.exp(heights), dims[dim] // shards_of).reshape((-1,) + (1,) * (len(dims) - dim - 1))

    gain = one(*pieces[0])
    for cut in pieces[1:]:
        gain = gain * one(*cut)
    return gain


def centred(stream_key, extent, scale, bound, cuts=(), kind=jnp.bfloat16):
    gain = steps_of(stream_key, extent, cuts, -0.22, 0.18) if cuts else 1.0
    values = jax.random.normal(stream_key, extent, jnp.float32) * scale * gain
    return jnp.minimum(jnp.maximum(values, -bound), bound).astype(kind)


def setup_inputs(seed: int = 0) -> dict:
    seeds = jax.random.split(jax.random.key(seed), 19)
    tokens = centred(seeds[0], (STEP_COUNT, D), 1.0, 6.0, ((0, 16),))
    norm_gain = jnp.clip(1.0 + 0.18 * jax.random.normal(seeds[1], (D,), jnp.float32), 0.1, 1.9)
    conv_value_weight = centred(seeds[2], (D, CONV_W), D ** -0.5, 0.125, ((0, 16), (1, 2)))
    conv_gate_weight = centred(seeds[3], (D, CONV_W), D ** -0.5, 0.125, ((0, 16), (1, 2)))
    conv_kernel = draw_conv_kernel(jax.random.fold_in(seeds[18], 71), 0)
    conv_bias = centred(seeds[5], (CONV_W,), 1.0, 4.0, ((0, 2),), jnp.float32)
    channel_gain = jnp.clip(1.0 + 0.18 * jax.random.normal(seeds[6], (CONV_W,), jnp.float32), 0.1, 1.9)
    query_weight = centred(seeds[7], (D, MEMORY_GROUPS * KEY_DIM), D ** -0.5, 0.125, ((0, 16), (1, 2)))
    key_weight = centred(seeds[8], (D, MEMORY_GROUPS * KEY_DIM), D ** -0.5, 0.125, ((0, 16), (1, 2)))
    value_weight = centred(seeds[9], (D, MEMORY_GROUPS * VALUE_DIM), D ** -0.5, 0.125, ((0, 16), (1, 2)))
    gate_weight = centred(seeds[10], (D, 4 * MEMORY_GROUPS), D ** -0.5, 0.125)
    gate_offset = draw_gate_offset(jax.random.fold_in(seeds[18], 71), 0)
    start_memory = centred(seeds[12], (2, MEMORY_GROUPS, VALUE_DIM, KEY_DIM), KEY_DIM ** -0.5, 0.375, ((1, 2),), jnp.float32)
    start_norm = centred(seeds[13], (2, MEMORY_GROUPS, KEY_DIM), KEY_DIM ** -0.5, 0.375, ((1, 2),), jnp.float32)
    start_level = jnp.clip(2.0 + 3.0 * jax.random.uniform(seeds[14], (2, MEMORY_GROUPS), jnp.float32) ** steps_of(seeds[14], (2, MEMORY_GROUPS), ((1, 2),), -0.2, 0.2), 2.0, 5.0)
    cell_gain = jnp.clip(1.0 + 0.18 * jax.random.normal(seeds[15], (MEMORY_GROUPS * VALUE_DIM,), jnp.float32), 0.1, 1.9)
    out_conv_weight = centred(seeds[16], (D, CONV_W), (CONV_W // 2) ** -0.5, 0.25, ((0, 16), (1, 2)))
    out_cell_weight = centred(seeds[17], (D, MEMORY_GROUPS * VALUE_DIM), (MEMORY_GROUPS * VALUE_DIM) ** -0.5, 0.09375, ((0, 16), (1, 2)))
    return {"tokens": tokens, "norm_gain": norm_gain, "conv_value_weight": conv_value_weight, "conv_gate_weight": conv_gate_weight, "conv_kernel": conv_kernel, "conv_bias": conv_bias, "channel_gain": channel_gain, "query_weight": query_weight, "key_weight": key_weight, "value_weight": value_weight, "gate_weight": gate_weight, "gate_offset": gate_offset, "start_memory": start_memory, "start_norm": start_norm, "start_level": start_level, "cell_gain": cell_gain, "out_conv_weight": out_conv_weight, "out_cell_weight": out_cell_weight}


EPS = 1e-06
HIGHEST = lax.Precision.HIGHEST

def back_to_wide(values):
    return lax.optimization_barrier(values.astype(jnp.bfloat16)).astype(jnp.float32)

def block_step(carried, inputs):
    memory, normer, run_level = carried
    queries, key_rows, value_rows, in_gate, log_forget = inputs
    length = queries.shape[0]
    lower_mask = jnp.arange(length)[:, None] >= jnp.arange(length)[None, :]
    cumulative = jnp.cumsum(log_forget)
    decay_table = jnp.where(lower_mask, cumulative[:, None] - cumulative[None, :] + in_gate[None, :], -jnp.inf)
    carried_level = cumulative + run_level
    top_level = jnp.maximum(carried_level, lax.optimization_barrier(jnp.max(decay_table, axis=1)))
    carry_weight = jnp.exp(carried_level - top_level)
    scores = jnp.dot(queries, key_rows.T, precision=HIGHEST) * jnp.exp(decay_table - top_level[:, None])
    numerator = jnp.dot(scores, value_rows, precision=HIGHEST) + carry_weight[:, None] * jnp.dot(queries, memory.T, precision=HIGHEST)
    denominator = lax.optimization_barrier(jnp.sum(scores, axis=1)) + carry_weight * jnp.dot(queries, normer, precision=HIGHEST)
    outputs = numerator / jnp.maximum(jnp.abs(denominator), 1.0)[:, None]
    block_total = cumulative[-1]
    tail_level = block_total - cumulative + in_gate
    new_level = jnp.maximum(block_total + run_level, jnp.max(tail_level))
    old_weight = jnp.exp(block_total + run_level - new_level)
    new_weight = jnp.exp(tail_level - new_level)
    memory = old_weight * memory + jnp.dot((value_rows * new_weight[:, None]).T, key_rows, precision=HIGHEST)
    normer = old_weight * normer + jnp.dot(new_weight, key_rows, precision=HIGHEST)
    return ((memory, normer, new_level), outputs)

def run_cell(queries, key_rows, value_rows, in_gate, log_forget, memory, normer, run_level):
    blocks = queries.shape[0] // BLOCK

    def to_blocks(values):
        return values.reshape((blocks, BLOCK) + values.shape[1:])
    final_state, outputs = lax.scan(block_step, (memory, normer, run_level), tuple((to_blocks(values) for values in (queries, key_rows, value_rows, in_gate, log_forget))))
    return outputs.reshape(queries.shape[0], value_rows.shape[1])

def head_outputs(inputs):
    queries, key_rows, value_rows, in_gate, log_forget, memory, normer, run_level = inputs
    forward = run_cell(queries, key_rows, value_rows, in_gate[0], log_forget[0], memory[0], normer[0], run_level[0])
    backward = run_cell(queries[::-1], key_rows[::-1], value_rows[::-1], in_gate[1, ::-1], log_forget[1, ::-1], memory[1], normer[1], run_level[1])[::-1]
    both_ways = forward + backward
    return both_ways * lax.rsqrt(lax.optimization_barrier(jnp.mean(both_ways * both_ways, axis=1, keepdims=True)) + EPS)

def reference(tokens, norm_gain, conv_value_weight, conv_gate_weight, conv_kernel, conv_bias, channel_gain, query_weight, key_weight, value_weight, gate_weight, gate_offset, start_memory, start_norm, start_level, cell_gain, out_conv_weight, out_cell_weight):
    features = tokens.astype(jnp.float32)
    normed = (features * lax.rsqrt(lax.optimization_barrier(jnp.mean(features * features, axis=1, keepdims=True)) + EPS) * norm_gain).astype(jnp.bfloat16)

    def project(weight):
        return jnp.dot(normed, weight, preferred_element_type=jnp.float32)
    conv_value = project(conv_value_weight).astype(jnp.bfloat16)
    conv_gate = project(conv_gate_weight).astype(jnp.bfloat16)
    gated_rows = (conv_value.astype(jnp.float32) * jax.nn.sigmoid(conv_gate.astype(jnp.float32))).astype(jnp.bfloat16)
    half_reach = KERNEL // 2
    padded = jnp.pad(gated_rows.astype(jnp.float32), ((half_reach, half_reach), (0, 0)))
    conv_sum = conv_bias + sum((conv_kernel[offset] * padded[offset:offset + STEP_COUNT] for offset in range(KERNEL)))
    channel_mean = lax.optimization_barrier(jnp.mean(conv_sum, axis=1, keepdims=True))
    channel_var = lax.optimization_barrier(jnp.mean(conv_sum * conv_sum, axis=1, keepdims=True)) - channel_mean * channel_mean
    conv_out = jax.nn.silu((conv_sum - channel_mean) * lax.rsqrt(channel_var + EPS) * channel_gain).astype(jnp.bfloat16)

    def split_heads(flat_rows, head_width):
        return jnp.transpose(back_to_wide(flat_rows).reshape(STEP_COUNT, MEMORY_GROUPS, head_width), (1, 0, 2))
    queries = split_heads(project(query_weight), KEY_DIM)
    key_rows = split_heads(project(key_weight), KEY_DIM) * KEY_DIM ** (-0.5)
    value_rows = split_heads(project(value_weight), VALUE_DIM)
    gate_pre = project(gate_weight).reshape(STEP_COUNT, 2, 2, MEMORY_GROUPS)
    gate_pre = jnp.transpose(gate_pre, (1, 2, 3, 0)) + gate_offset
    in_gate = jnp.transpose(gate_pre[:, 0], (1, 0, 2))
    log_forget = jnp.transpose(jax.nn.log_sigmoid(gate_pre[:, 1]), (1, 0, 2))
    cells = lax.map(head_outputs, (queries, key_rows, value_rows, in_gate, log_forget, jnp.transpose(start_memory, (1, 0, 2, 3)), jnp.transpose(start_norm, (1, 0, 2)), jnp.transpose(start_level, (1, 0))))
    cell_out = (jnp.transpose(cells, (1, 0, 2)).reshape(STEP_COUNT, MEMORY_GROUPS * VALUE_DIM) * cell_gain).astype(jnp.bfloat16)
    conv_groups = conv_out.reshape(STEP_COUNT, N_TP, CONV_W // N_TP)
    cell_groups = cell_out.reshape(STEP_COUNT, N_TP, MEMORY_GROUPS * VALUE_DIM // N_TP)
    conv_weights = out_conv_weight.reshape(D, N_TP, CONV_W // N_TP)
    cell_weights = out_cell_weight.reshape(D, N_TP, MEMORY_GROUPS * VALUE_DIM // N_TP)
    mixed_sum = jnp.zeros((STEP_COUNT, D), jnp.float32)
    for group in range(N_TP):
        partial_value = jnp.einsum('tc,dc->td', conv_groups[:, group], conv_weights[:, group], preferred_element_type=jnp.float32) + jnp.einsum('tc,dc->td', cell_groups[:, group], cell_weights[:, group], preferred_element_type=jnp.float32)
        mixed_sum = mixed_sum + lax.optimization_barrier(partial_value.astype(jnp.bfloat16)).astype(jnp.float32)
    return mixed_sum.astype(jnp.bfloat16)
```

```python
import math

import jax
import jax.numpy as jnp
from jax import lax
from jax.experimental import pallas as pl
from jax.experimental.pallas import tpu as pltpu
from jax.sharding import PartitionSpec as P

EPS = 1e-06
LOW = -1e30
F32 = jnp.float32
BF16 = jnp.bfloat16


def dot(a, b, dims=((1,), (0,))):
    return lax.dot_general(a, b, (dims, ((), ())), preferred_element_type=F32)


def pick(stack, index, axis=0):
    return lax.dynamic_index_in_dim(stack, index, axis, keepdims=False)


class Layout:
    def __init__(self, heads_here):
        self.S = lax.axis_size("sp")
        self.T = lax.axis_size("tp")
        self.C = math.gcd(heads_here, self.S)
        self.R = self.S // self.C
        s = lax.axis_index("sp")
        self.h = s // self.R
        self.q = s % self.R
        self.c = lax.axis_index("tp")

    def along_h(self, x, d):
        C, R = self.C, self.R
        return lax.ppermute(
            x, "sp", [(h * R + q, (h + d) % C * R + q) for h in range(C) for q in range(R)]
        )

    def along_q(self, x, d):
        C, R = self.C, self.R
        return lax.ppermute(
            x, "sp", [(h * R + q, h * R + (q + d) % R) for h in range(C) for q in range(R)]
        )

    def flip_q(self, x, d):
        C, R = self.C, self.R
        return lax.ppermute(
            x, "sp", [(h * R + q, h * R + (q ^ d)) for h in range(C) for q in range(R)]
        )

    def along_tp(self, x, d):
        T = self.T
        return lax.ppermute(x, "tp", [(c, (c + d) % T) for c in range(T)])

    def to_part(self, x, d):
        C, R = self.C, self.R
        return lax.ppermute(
            x, "sp", [(s, (s % C + d) % C * R + s // C) for s in range(self.S)]
        )

    def spread_heads(self, chunks_of):
        C = self.C
        got = [chunks_of(self.h)]
        for d in range(1, C):
            got.append(self.along_h(chunks_of((self.h + d) % C), d))
        rev = [got[(-k) % C] for k in range(C)]
        if C == 1:
            return rev[0][None]
        twice = jnp.stack(rev + rev)
        return lax.dynamic_slice_in_dim(twice, (C - self.h) % C, C, 0)

    def gather_parts(self, x):
        R = self.R
        n = x.shape[0]
        if R == 4 and n % 2 == 0:
            a = self.flip_q(x, 1)
            b = self.flip_q(x, 2)
            m = n // 2
            c = self.flip_q(a[:m], 2)
            d = self.flip_q(b[m:], 1)
            return [
                (self.q, 0, n, x),
                (self.q ^ 1, 0, n, a),
                (self.q ^ 2, 0, n, b),
                (self.q ^ 3, 0, m, c),
                (self.q ^ 3, m, n, d),
            ]
        if R <= 8:
            return [(self.q, 0, n, x)] + [
                ((self.q - d) % R, 0, n, self.along_q(x, d)) for d in range(1, R)
            ]
        groups = [[h * R + q for q in range(R)] for h in range(self.C)]
        g = lax.all_gather(x, "sp", axis=0, axis_index_groups=groups, tiled=False)
        return [(q, 0, n, g[q]) for q in range(R)]


def shards_general(
    tokens,
    norm_gain,
    conv_value_weight,
    conv_gate_weight,
    conv_kernel,
    conv_bias,
    channel_gain,
    query_weight,
    key_weight,
    value_weight,
    gate_weight,
    gate_offset,
    start_memory,
    start_norm,
    start_level,
    cell_gain,
    out_conv_weight,
    out_cell_weight,
):
    heads_here = start_level.shape[1]
    L = Layout(heads_here)
    S, T, C, R, h, q, c = L.S, L.T, L.C, L.R, L.h, L.q, L.c
    HL = heads_here // C
    B = tokens.shape[0]
    D = tokens.shape[1]
    N = B * C
    rows = D // S
    key_width = start_norm.shape[2]
    value_width = start_memory.shape[2]
    chan = conv_bias.shape[0] // C
    conv_all = conv_bias.shape[0] * T

    def mine(x, axis):
        n = x.shape[axis] // C
        return lax.dynamic_slice_in_dim(x, h * n, n, axis)

    features = tokens.astype(F32)
    normed = (
        features * lax.rsqrt(jnp.mean(features * features, axis=1, keepdims=True) + EPS) * norm_gain
    ).astype(BF16)
    normed = normed.reshape(B, C, R, rows).transpose(0, 2, 1, 3).reshape(B, D)
    half = D // T
    share = lax.dynamic_slice_in_dim(normed, c * half, half, 1)

    def columns(weights, line):
        return jnp.concatenate(
            [
                lax.dynamic_slice_in_dim(w, line * (w.shape[1] // C), w.shape[1] // C, 1)
                for w in weights
            ],
            axis=1,
        )

    def first(weights):
        got = L.spread_heads(lambda line: columns(weights, line))
        return got.reshape(C * rows, got.shape[2])

    conv_piece = first((conv_value_weight, conv_gate_weight))
    key_piece = first((key_weight,))
    value_piece = first((value_weight,))
    query_piece = first((query_weight,))

    got_tokens = [L.to_part(share, d) if C > 1 else share for d in range(C)]
    offsets = gate_offset.reshape(2, 2, C, HL, B)
    j_here = lax.axis_index("sp") % C
    got_offset = [
        L.to_part(pick(offsets, (j_here + d) % C, 2), d) if C > 1 else offsets[:, :, 0]
        for d in range(C)
    ]

    def in_order(got, axis):
        if C == 1:
            return got[0]
        rev = [got[(-k) % C] for k in range(C)]
        twice = jnp.concatenate(rev + rev, axis=axis)
        n = got[0].shape[axis]
        return lax.dynamic_slice_in_dim(twice, (C - h) % C * n, C * n, axis)

    share_all = in_order(got_tokens, 0)
    offset_all = in_order(got_offset, 3)
    others = [L.along_tp(share_all, d) for d in range(1, T)]
    parts = [share_all] + others
    rev = [parts[(-k) % T] for k in range(T)]
    hidden = lax.dynamic_slice_in_dim(
        jnp.concatenate(rev + rev, axis=1), (T - c) % T * half, D, 1
    )

    wide = C * rows

    def project(piece):
        total = None
        for part, lo, hi, w in L.gather_parts(piece):
            x = lax.dynamic_slice_in_dim(hidden, part * wide + lo, hi - lo, 1)
            y = dot(x, w)
            total = y if total is None else total + y
        return total

    conv_pre = project(conv_piece).astype(BF16)
    keys = project(key_piece).astype(BF16)
    values = project(value_piece).astype(BF16)
    queries = project(query_piece).astype(BF16)

    out_piece = L.spread_heads(
        lambda line: columns((out_conv_weight, out_cell_weight), line)
    ).reshape(C * rows, -1)
    out_rows = jnp.zeros((D, out_piece.shape[1]), BF16)
    for part, lo, hi, w in L.gather_parts(out_piece):
        out_rows = lax.dynamic_update_slice(out_rows, w, (part * wide + lo, 0))

    conv_value = conv_pre[:, :chan].astype(F32)
    conv_gate = conv_pre[:, chan:].astype(F32)
    gated = (conv_value * jax.nn.sigmoid(conv_gate)).astype(BF16)
    reach = conv_kernel.shape[0] // 2
    line_up = [(l * R + i, l * R + i + 1) for l in range(C) for i in range(R - 1)]
    before = lax.ppermute(gated[N - reach :], "sp", line_up)
    after = lax.ppermute(gated[:reach], "sp", [(b, a) for a, b in line_up])
    padded = jnp.concatenate([before, gated, after], axis=0).astype(F32)
    taps = mine(conv_kernel, 1)
    conv_sum = mine(conv_bias, 0) + sum(
        taps[k] * padded[k : k + N] for k in range(taps.shape[0])
    )
    stats = jnp.stack([jnp.sum(conv_sum, axis=1), jnp.sum(conv_sum * conv_sum, axis=1)])
    total = stats
    for d in range(C):
        for e in range(T):
            if d or e:
                total = total + lax.ppermute(
                    stats,
                    ("sp", "tp"),
                    [
                        ((l * R + p) * T + t, ((l + d) % C * R + p) * T + (t + e) % T)
                        for l in range(C)
                        for p in range(R)
                        for t in range(T)
                    ],
                )
    mean = total[0] / conv_all
    var = total[1] / conv_all - mean * mean
    conv_out = jax.nn.silu(
        (conv_sum - mean[:, None]) * lax.rsqrt(var + EPS)[:, None] * mine(channel_gain, 0)
    ).astype(BF16)

    groups = gate_weight.shape[1] // 4
    gates_w = gate_weight.reshape(C, R, rows, 4, groups)
    gates_w = lax.dynamic_slice_in_dim(gates_w, c * heads_here + h * HL, HL, 4)
    gates_w = gates_w.transpose(1, 0, 2, 3, 4).reshape(D, 4 * HL)
    gate_pre = dot(gates_w, hidden, ((0,), (1,))).reshape(2, 2, HL, N) + offset_all
    in_gate = gate_pre[:, 0]
    log_forget = jax.nn.log_sigmoid(gate_pre[:, 1])
    upto = (jnp.arange(N)[:, None] <= jnp.arange(N)[None, :]).astype(F32)
    forward_sum = jnp.dot(log_forget[0], upto, precision=lax.Precision.HIGHEST)
    backward_sum = jnp.dot(log_forget[1], upto.T, precision=lax.Precision.HIGHEST)
    sums = jnp.stack([forward_sum, backward_sum])
    passed = jnp.stack([forward_sum[:, -1], backward_sum[:, 0]])
    tail = passed[:, :, None] - sums + in_gate
    level = jnp.max(tail, axis=2)
    new_weight = jnp.exp(tail - level[:, :, None])
    my_memory = mine(start_memory, 1)
    my_norm = mine(start_norm, 1)
    my_level = mine(start_level, 1)
    step = jnp.arange(N)
    cells = []
    scale = key_width ** (-0.5)
    for i in range(HL):
        k = keys[:, i * key_width : (i + 1) * key_width] * jnp.asarray(scale, BF16)
        v = values[:, i * value_width : (i + 1) * value_width]
        qr = queries[:, i * key_width : (i + 1) * key_width]
        memories = []
        norms = []
        for d in range(2):
            w = new_weight[d, i]
            memories.append(dot((v.astype(F32) * w[:, None]).astype(BF16), k, ((0,), (0,))))
            norms.append(jnp.sum(w[:, None] * k.astype(F32), axis=0))
        memories = jnp.stack(memories).astype(BF16)
        smalls = jnp.concatenate(
            [jnp.stack(norms), level[:, i, None], passed[:, i, None]], axis=1
        )
        if R <= 8:
            got = []
            for d in range(1, R):
                back = jnp.where(q + d < R, 0, 1)
                got.append(
                    (L.along_q(pick(memories, back), d), L.along_q(pick(smalls, back), d))
                )
            get = lambda direction, dist: got[dist - 1 if direction == 0 else R - dist - 1]
        else:
            groups_q = [[l * R + p for p in range(R)] for l in range(C)]
            all_m = lax.all_gather(memories, "sp", axis=0, axis_index_groups=groups_q)
            all_s = lax.all_gather(smalls, "sp", axis=0, axis_index_groups=groups_q)

            def get(direction, dist):
                p = (q - dist) % R if direction == 0 else (q + dist) % R
                return pick(all_m, p)[direction], pick(all_s, p)[direction]

        mixed_rows = None
        scores = dot(qr, k, ((1,), (1,)))
        table_sum = None
        carried = None
        for direction in range(2):
            levels, mems, nrms = [], [], []
            decay = jnp.zeros((), F32)
            for dist in range(1, R):
                m, sm = get(direction, dist)
                there = q >= dist if direction == 0 else q + dist < R
                levels.append(jnp.where(there, sm[-2] + decay, LOW))
                mems.append(m)
                nrms.append(sm[:-2])
                decay = decay + jnp.where(there, sm[-1], 0.0)
            levels.append(my_level[direction, i] + decay)
            mems.append(my_memory[direction, i])
            nrms.append(my_norm[direction, i])
            run_level = levels[0]
            for lv in levels[1:]:
                run_level = jnp.maximum(run_level, lv)
            ws = [jnp.exp(lv - run_level) for lv in levels]
            memory = sum(w * m.astype(F32) for w, m in zip(ws, mems)).astype(BF16)
            norm = sum(w * n for w, n in zip(ws, nrms))
            f = sums[direction, i]
            g = in_gate[direction, i]
            mask = step[:, None] >= step[None, :] if direction == 0 else step[:, None] <= step[None, :]
            table = jnp.where(mask, f[:, None] + (g - f)[None, :], -jnp.inf)
            entry = f + run_level
            top = jnp.maximum(jnp.max(table, axis=1), entry)
            weights = scores * jnp.exp(table - top[:, None])
            ew = jnp.exp(entry - top)
            qn = jnp.sum(qr.astype(F32) * norm[None, :], axis=1)
            den = jnp.sum(weights, axis=1) + ew * qn
            inv = 1.0 / jnp.maximum(jnp.abs(den), 1.0)
            scaled = weights * inv[:, None]
            table_sum = scaled if table_sum is None else table_sum + scaled
            part = dot(qr, memory, ((1,), (1,))) * (ew * inv)[:, None]
            carried = part if carried is None else carried + part
        both = dot(table_sum.astype(BF16), v) + carried
        both = both * lax.rsqrt(jnp.mean(both * both, axis=1, keepdims=True) + EPS)
        gain = lax.dynamic_slice_in_dim(mine(cell_gain, 0), i * value_width, value_width, 0)
        cells.append((both * gain).astype(BF16))

    act = jnp.concatenate([conv_out] + cells, axis=1)
    strip = B // T
    act = act.reshape(C, T, strip, act.shape[1])

    def rows_for(t):
        x = pick(act, t, 1).reshape(C * strip, act.shape[3])
        return dot(x, out_rows, ((1,), (1,)))

    arrived = [L.along_tp(rows_for((c + d) % T).astype(BF16), d) for d in range(1, T)]
    own = rows_for(c)
    for a in arrived:
        own = own + a.astype(F32)
    blocks = own.astype(BF16).reshape(C, strip, D)

    if C == 1:
        final = blocks[0].astype(F32)
    elif C == R:
        got = [pick(blocks, q)]
        for d in range(1, R):
            got.append(L.along_q(pick(blocks, (q + d) % R), d))
        rev = [got[(-k) % R] for k in range(R)]
        by_part = jnp.stack(rev)
        final = pick(by_part, (h - q) % R).astype(F32)
        for d in range(1, C):
            final = final + L.along_h(pick(by_part, (h + d - q) % R), d).astype(F32)
    else:
        final = 0.0
        for d in range(C):
            perm = [(l * R + p, p * C + (l + d) % C) for l in range(C) for p in range(R)]
            final = final + lax.ppermute(pick(blocks, (h + d) % C), "sp", perm).astype(F32)
    final = final.astype(BF16).reshape(strip, R, C, rows).transpose(0, 2, 1, 3)
    return final.reshape(strip, D)

VMEM = pl.BlockSpec(memory_space=pltpu.VMEM)
SMEM = pl.BlockSpec(memory_space=pltpu.SMEM)
HIGHEST = lax.Precision.HIGHEST
NT = ((1,), (1,))
TN = ((0,), (0,))


def kernel(body, outs, *args, scratch=(), name=None, limit=48 << 20):
    shapes = [jax.ShapeDtypeStruct(s, d) for s, d in outs]
    return pl.pallas_call(
        body,
        out_shape=shapes if len(shapes) > 1 else shapes[0],
        in_specs=[SMEM] + [VMEM] * (len(args) - 1),
        out_specs=[VMEM] * len(shapes) if len(shapes) > 1 else VMEM,
        scratch_shapes=scratch,
        compiler_params=pltpu.CompilerParams(vmem_limit_bytes=limit),
        name=name,
    )(*args)


def three(x):
    a = x.astype(BF16).astype(F32)
    b = (x - a).astype(BF16).astype(F32)
    return a, b, x - a - b


def norm_body(pos, tok, gain, off, share):
    C, R = 4, 4
    B, D = tok.shape
    rows = D // (C * R)
    x = tok[...].astype(F32)
    y = x * lax.rsqrt(jnp.mean(x * x, axis=1, keepdims=True) + EPS) * gain[...]
    y = y.astype(BF16)
    halves = []
    for t in range(2):
        halves.append(
            jnp.concatenate(
                [
                    y[:, (hh * R + qq) * rows : (hh * R + qq + 1) * rows]
                    for qq in (2 * t, 2 * t + 1)
                    for hh in range(C)
                ],
                axis=1,
            )
        )
    share[0:B, :] = jnp.where(pos[2] == 0, halves[0], halves[1])
    o = jnp.concatenate([off[k] for k in range(4)], axis=1)
    a, b, c = three(o)
    extra = jnp.concatenate(
        [jnp.concatenate([a, b], axis=1), jnp.concatenate([c, jnp.zeros_like(c)], axis=1)], axis=0
    )
    extra = jnp.concatenate([extra, jnp.zeros_like(extra)], axis=0)
    share[B : B + 16, :] = extra.astype(BF16)


def arrange_body(pos, g0, g1, g2, g3, own, offs):
    h = pos[0]
    B = own.shape[1]
    for d, g in enumerate((g0, g1, g2, g3)):
        j = lax.rem(h - d + 4, 4)
        own[j] = g[0:B, :]
        e = g[B : B + 16, :].astype(F32)
        row = lax.broadcasted_iota(jnp.int32, e.shape, 0)
        ab = jnp.sum(jnp.where(row == h, e, 0.0), axis=0, keepdims=True)
        cc = jnp.sum(jnp.where(row == h + 4, e, 0.0), axis=0, keepdims=True)
        n = ab.shape[1] // 2
        o = ab[:, :n] + ab[:, n:] + cc[:, :n]
        for k in range(4):
            offs[j, k : k + 1, :] = o[:, k * B : (k + 1) * B]


def fill_hidden(pos, own, other, hid):
    c = pos[2]
    n = own.shape[1] // 2
    for i in range(2):
        hid[2 * c + i] = own[:, i * n : (i + 1) * n]
        hid[2 - 2 * c + i] = other[:, i * n : (i + 1) * n]


def projected(pos, hid, x0, xa, xb, xc, xd):
    q = pos[1]
    m = xc.shape[0]
    y = dot(hid[q], x0[...]) + dot(hid[q ^ 1], xa[...]) + dot(hid[q ^ 2], xb[...])
    last = hid[q ^ 3]
    return y + dot(last[:, :m], xc[...]) + dot(last[:, m:], xd[...])


def row_of(x, rows, r):
    return x[r : r + 1, :]


def state_body(pos, own, other, x0, xa, xb, xc, xd, gw, offs, k_out, v_out, g_out, msg, hid):
    q = pos[1]
    fill_hidden(pos, own, other, hid)
    y = projected(pos, hid, x0, xa, xb, xc, xd)
    kw = k_out.shape[1]
    N = y.shape[0]
    k = (y[:, :kw].astype(BF16).astype(F32) * (kw ** (-0.5))).astype(BF16)
    v = y[:, kw:].astype(BF16)
    k_out[...] = k
    v_out[...] = v
    pre = None
    for p in range(4):
        t = dot(gw[p], hid[p], NT)
        pre = t if pre is None else pre + t
    off = jnp.concatenate([offs[j] for j in range(4)], axis=1)
    pre = pre[0:4, :] + off
    lf = jnp.minimum(pre, 0.0) - jnp.log1p(jnp.exp(-jnp.abs(pre)))
    lf8 = jnp.concatenate([lf, lf], axis=0)
    ri = lax.broadcasted_iota(jnp.int32, (N, N), 0)
    ci = lax.broadcasted_iota(jnp.int32, (N, N), 1)
    up = jnp.where(ri <= ci, 1.0, 0.0)
    down = jnp.where(ri >= ci, 1.0, 0.0)
    f = jnp.dot(lf8, up, precision=HIGHEST)[1:2]
    b = jnp.dot(lf8, down, precision=HIGHEST)[3:4]
    inf, inb = pre[0:1], pre[2:3]
    pf, pb = f[:, N - 1 : N], b[:, 0:1]
    tf, tb = pf - f + inf, pb - b + inb
    lvf, lvb = jnp.max(tf, axis=1, keepdims=True), jnp.max(tb, axis=1, keepdims=True)
    wf, wb = jnp.exp(tf - lvf), jnp.exp(tb - lvb)
    zero = jnp.zeros_like(f)
    g_out[...] = jnp.concatenate([f, b, inf - f, inb - b, zero, zero, zero, zero], axis=0)
    w8 = jnp.concatenate([wf, wb, zero, zero, zero, zero, zero, zero], axis=0)
    wt = w8.T
    nn = jnp.dot(w8, k.astype(F32), precision=HIGHEST)
    v32 = v.astype(F32)
    mf = dot((v32 * wt[:, 0:1]).astype(BF16), k, TN).astype(BF16)
    mb = dot((v32 * wt[:, 1:2]).astype(BF16), k, TN).astype(BF16)
    def small(n, lv, ps):
        wide = lambda z: jnp.broadcast_to(z, n.shape)
        r = list(three(n)) + [wide(z) for z in three(lv)] + [wide(z) for z in three(ps)]
        return jnp.concatenate(r + [jnp.zeros((7, n.shape[1]), F32)], axis=0).astype(BF16)
    sf, sb = small(nn[0:1], lvf, pf), small(nn[1:2], lvb, pb)
    vw = mf.shape[0]
    for p in range(4):
        @pl.when(p > q)
        def _():
            msg[p, 0:vw, :] = mf
            msg[p, vw : vw + 16, :] = sf
        @pl.when(p <= q)
        def _():
            msg[p, 0:vw, :] = mb
            msg[p, vw : vw + 16, :] = sb


def gate_body(pos, own, other, x0, xa, xb, xc, xd, gated, head, tail, q_out, hid):
    fill_hidden(pos, own, other, hid)
    y = projected(pos, hid, x0, xa, xb, xc, xd)
    n = gated.shape[1]
    a = y[:, :n].astype(BF16).astype(F32)
    g = y[:, n : 2 * n].astype(BF16).astype(F32)
    z = (a * jax.nn.sigmoid(g)).astype(BF16)
    gated[...] = z
    head[...] = z[0:16, :]
    tail[...] = z[z.shape[0] - 16 :, :]
    q_out[...] = y[:, 2 * n :].astype(BF16)


def conv_body(pos, gated, before, after, taps, bias, conv, stats, pad):
    N, n = gated.shape
    K = taps.shape[0]
    pad[0:16, :] = before[...].astype(F32)
    pad[16 : 16 + N, :] = gated[...].astype(F32)
    pad[16 + N : 32 + N, :] = after[...].astype(F32)
    lo = 16 - K // 2
    step = 64
    for r in range(0, N, step):
        acc = jnp.broadcast_to(bias[...], (step, n))
        for k in range(K):
            acc = acc + taps[k : k + 1, :] * pad[lo + k + r : lo + k + r + step, :]
        conv[r : r + step, :] = acc
    x = conv[...]
    ones = jnp.ones((8, n), F32)
    s1 = lax.dot_general(ones, x, (NT, ((), ())), precision=HIGHEST, preferred_element_type=F32)
    s2 = lax.dot_general(ones, x * x, (NT, ((), ())), precision=HIGHEST, preferred_element_type=F32)
    row = lax.broadcasted_iota(jnp.int32, s1.shape, 0)
    both = jnp.where(row == 0, s1, s2)
    for i in range(stats.shape[0]):
        stats[i] = both


def cell_body(pos, qr, k, v, g, msg, mem0, nrm0, lev0, gain, conv, stats, chgain, act):
    q = pos[1]
    N, kw = qr.shape
    vw = v.shape[1]
    n = conv.shape[1]
    lv, ps, nr = [], [], []
    for p in range(4):
        e = msg[p, vw : vw + 16, :].astype(F32)
        nr.append(e[0:1] + e[1:2] + e[2:3])
        lv.append((e[3:4] + e[4:5] + e[5:6])[:, 0:1])
        ps.append((e[6:7] + e[7:8] + e[8:9])[:, 0:1])
    mems, nrms, runs = [], [], []
    for d in range(2):
        def ok(p):
            return p < q if d == 0 else p > q
        lvs = []
        for p in range(4):
            between = range(p + 1, 4) if d == 0 else range(0, p)
            x = lv[p]
            for m in between:
                x = x + jnp.where(ok(m), ps[m], 0.0)
            lvs.append(jnp.where(ok(p), x, LOW))
        x = lev0[d : d + 1, 0:1]
        for m in range(4):
            x = x + jnp.where(ok(m), ps[m], 0.0)
        lvs.append(x)
        run = lvs[0]
        for y in lvs[1:]:
            run = jnp.maximum(run, y)
        ws = [jnp.exp(y - run) for y in lvs]
        mm = ws[4] * mem0[d]
        nm = ws[4] * nrm0[d : d + 1, :]
        for p in range(4):
            mm = mm + ws[p] * msg[p, 0:vw, :].astype(F32)
            nm = nm + ws[p] * nr[p]
        mems.append(mm.astype(BF16))
        nrms.append(nm)
        runs.append(run)
    gt = g[...].T
    st = stats[0]
    for i in range(1, stats.shape[0]):
        st = st + stats[i]
    width = n * stats.shape[0]
    mean = st[0:1] / width
    var = st[1:2] / width - mean * mean
    mv = jnp.concatenate([mean, lax.rsqrt(var + EPS)] + [jnp.zeros_like(mean)] * 6, axis=0).T
    blk = N // 4
    half = blk // 2
    for j in range(4):
        r0 = j * blk
        qb = qr[r0 : r0 + blk, :]
        q32 = qb.astype(F32)
        scores = dot(qb, k[...], NT)
        ri = lax.broadcasted_iota(jnp.int32, (blk, N), 0) + r0
        ci = lax.broadcasted_iota(jnp.int32, (blk, N), 1)
        total, both = None, None
        for d in range(2):
            fc = gt[r0 : r0 + blk, d : d + 1]
            mask = ri >= ci if d == 0 else ri <= ci
            table = jnp.where(mask, fc + g[2 + d : 3 + d, :], -jnp.inf)
            entry = fc + runs[d]
            top = jnp.maximum(jnp.max(table, axis=1, keepdims=True), entry)
            w = scores * jnp.exp(table - top)
            ew = jnp.exp(entry - top)
            den = jnp.sum(w, axis=1, keepdims=True)
            den = den + ew * jnp.sum(q32 * nrms[d], axis=1, keepdims=True)
            inv = 1.0 / jnp.maximum(jnp.abs(den), 1.0)
            w = w * inv
            total = w if total is None else total + w
            part = dot(qb, mems[d], NT) * (ew * inv)
            both = part if both is None else both + part
        both = both + dot(total.astype(BF16), v[...])
        both = both * lax.rsqrt(jnp.mean(both * both, axis=1, keepdims=True) + EPS) * gain[...]
        both = both.astype(BF16)
        x = conv[r0 : r0 + blk, :]
        x = (x - mv[r0 : r0 + blk, 0:1]) * mv[r0 : r0 + blk, 1:2] * chgain[...]
        x = (x * jax.nn.sigmoid(x)).astype(BF16)
        for t in range(2):
            o = slice(j * half, (j + 1) * half)
            i = slice(t * half, (t + 1) * half)
            act[t, o, 0:n] = x[i]
            act[t, o, n:] = both[i]


def out_body(pos, act, x0, xa, xb, xc, xd, give, keep, wn):
    q, c = pos[1], pos[2]
    m = xc.shape[0]
    wn[q] = x0[...]
    wn[q ^ 1] = xa[...]
    wn[q ^ 2] = xb[...]
    wn[q ^ 3, 0:m, :] = xc[...]
    wn[q ^ 3, m:, :] = xd[...]
    w = x0.shape[0]
    for p in range(4):
        give[:, p * w : (p + 1) * w] = dot(act[1 - c], wn[p], NT).astype(BF16)
        keep[:, p * w : (p + 1) * w] = dot(act[c], wn[p], NT)


def last_body(pos, got, out):
    x = got[0].astype(F32)
    for i in range(1, got.shape[0]):
        x = x + got[i].astype(F32)
    x = x.astype(BF16)
    rows = x.shape[1] // 16
    for p in range(4):
        for l in range(4):
            s, t = (l * 4 + p) * rows, (p * 4 + l) * rows
            out[:, s : s + rows] = x[:, t : t + rows]


def shards(
    tokens,
    norm_gain,
    conv_value_weight,
    conv_gate_weight,
    conv_kernel,
    conv_bias,
    channel_gain,
    query_weight,
    key_weight,
    value_weight,
    gate_weight,
    gate_offset,
    start_memory,
    start_norm,
    start_level,
    cell_gain,
    out_conv_weight,
    out_cell_weight,
):
    heads_here = start_level.shape[1]
    L = Layout(heads_here)
    S, T, C, R, h, q, c = L.S, L.T, L.C, L.R, L.h, L.q, L.c
    B, D = tokens.shape
    N = B * C
    rows = D // S
    kw = start_norm.shape[2]
    vw = start_memory.shape[2]
    n = conv_bias.shape[0] // C
    fits = C == R == 4 and T == 2 and heads_here == C and B % 128 == 0 and rows % 128 == 0
    fits = fits and n % 128 == 0 and kw % 128 == 0 and vw % 128 == 0 and conv_kernel.shape[0] <= 31
    if not fits:
        return shards_general(
            tokens,
            norm_gain,
            conv_value_weight,
            conv_gate_weight,
            conv_kernel,
            conv_bias,
            channel_gain,
            query_weight,
            key_weight,
            value_weight,
            gate_weight,
            gate_offset,
            start_memory,
            start_norm,
            start_level,
            cell_gain,
            out_conv_weight,
            out_cell_weight,
        )
    pos = jnp.stack([h, q, c, jnp.zeros_like(h)]).astype(jnp.int32)
    lines = [[l * R + p for l in range(C)] for p in range(R)]
    planes = [[l * R + p for p in range(R)] for l in range(C)]

    def swap(x, groups, axes="sp"):
        return lax.all_to_all(x, axes, 0, 0, axis_index_groups=groups, tiled=True)

    def by_line(*weights):
        return jnp.concatenate(
            [w.reshape(rows, C, w.shape[1] // C).transpose(1, 0, 2) for w in weights], axis=2
        )

    def mine(x, axis):
        m = x.shape[axis] // C
        return lax.dynamic_slice_in_dim(x, h * m, m, axis)

    state_w = swap(by_line(key_weight, value_weight), lines).reshape(C * rows, -1)
    off = gate_offset.reshape(4, heads_here, B)
    share = kernel(
        norm_body, [((B + 16, D // 2), BF16)], pos, tokens, norm_gain.reshape(1, D), off, name="norm"
    )
    gate_w = swap(by_line(conv_value_weight, conv_gate_weight, query_weight), lines)
    gate_w = gate_w.reshape(C * rows, -1)
    got = [L.to_part(share, d) for d in range(C)]

    def pieces(x):
        return [p[3] for p in L.gather_parts(x)]

    state_p = pieces(state_w)
    own, offs = kernel(
        arrange_body,
        [((C, B, D // 2), BF16), ((C, 4, B), F32)],
        pos,
        *got,
        name="arrange",
    )
    own = own.reshape(N, D // 2)
    other = L.along_tp(own, 1)
    gate_p = pieces(gate_w)
    groups = gate_weight.shape[1] // 4
    gw = gate_weight.reshape(C, R, rows, 4, groups)
    gw = pick(gw, c * heads_here + h, 4).transpose(1, 3, 0, 2).reshape(R, 4, C * rows)
    gw = jnp.pad(gw, ((0, 0), (0, 4), (0, 0)))
    hid = pltpu.VMEM((R, N, C * rows), BF16)
    keys, values, gates, msg = kernel(
        state_body,
        [((N, kw), BF16), ((N, vw), BF16), ((8, N), F32), ((R, vw + 16, kw), BF16)],
        pos,
        own,
        other,
        *state_p,
        gw,
        offs,
        scratch=[hid],
        name="state",
    )
    msg = swap(msg, planes)
    gated, head, tail, queries = kernel(
        gate_body,
        [((N, n), BF16), ((16, n), BF16), ((16, n), BF16), ((N, kw), BF16)],
        pos,
        own,
        other,
        *gate_p,
        scratch=[hid],
        name="gate",
    )
    up = [(l * R + i, l * R + i + 1) for l in range(C) for i in range(R - 1)]
    before = lax.ppermute(tail, "sp", up)
    after = lax.ppermute(head, "sp", [(b, a) for a, b in up])
    conv, stats = kernel(
        conv_body,
        [((N, n), F32), ((C * T, 8, N), F32)],
        pos,
        gated,
        before,
        after,
        mine(conv_kernel, 1),
        mine(conv_bias, 0).reshape(1, n),
        scratch=[pltpu.VMEM((N + 32, n), F32)],
        name="conv",
    )
    stats = swap(
        stats,
        [[(l * R + p) * T + t for l in range(C) for t in range(T)] for p in range(R)],
        ("sp", "tp"),
    )
    out_w = swap(by_line(out_conv_weight, out_cell_weight), lines).reshape(C * rows, -1)
    out_p = pieces(out_w)
    act = kernel(
        cell_body,
        [((2, N // 2, n + vw), BF16)],
        pos,
        queries,
        keys,
        values,
        gates,
        msg,
        pick(start_memory, h, 1),
        pick(start_norm, h, 1),
        jnp.broadcast_to(pick(start_level, h, 1)[:, None], (2, 128)),
        mine(cell_gain, 0).reshape(1, vw),
        conv,
        stats,
        mine(channel_gain, 0).reshape(1, n),
        name="cell",
    )
    give, keep = kernel(
        out_body,
        [((N // 2, D), BF16), ((N // 2, D), F32)],
        pos,
        act,
        *out_p,
        scratch=[pltpu.VMEM((R, C * rows, n + vw), BF16)],
        name="out",
    )
    block = (keep + L.along_tp(give, 1).astype(F32)).astype(BF16).reshape(C, B // T, D)
    block = swap(swap(block, planes), lines)
    return kernel(last_body, [((B // T, D), BF16)], pos, block, name="last")


def solution(mesh):
    in_specs = (
        P("sp", None),
        P(),
        P("sp", "tp"),
        P("sp", "tp"),
        P(None, "tp"),
        P("tp"),
        P("tp"),
        P("sp", "tp"),
        P("sp", "tp"),
        P("sp", "tp"),
        P(),
        P(None, None, "tp", "sp"),
        P(None, "tp", None, None),
        P(None, "tp", None),
        P(None, "tp"),
        P("tp"),
        P("sp", "tp"),
        P("sp", "tp"),
    )
    out_specs = P(("sp", "tp"), None)
    return jax.shard_map(shards, mesh=mesh, in_specs=in_specs, out_specs=out_specs, check_vma=False)
```

```python
import math

import jax
import jax.numpy as jnp
from jax import lax
from jax.experimental import pallas as pl
from jax.experimental.pallas import tpu as pltpu
from jax.sharding import PartitionSpec as P


EPS = 1e-06
LOW = -1e30
F32 = jnp.float32
BF16 = jnp.bfloat16


def dot(a, b, dims=((1,), (0,))):
    return lax.dot_general(a, b, (dims, ((), ())), preferred_element_type=F32)


def pick(stack, index, axis=0):
    return lax.dynamic_index_in_dim(stack, index, axis, keepdims=False)


class Layout:
    def __init__(self, heads_here):
        self.S = lax.axis_size("sp")
        self.T = lax.axis_size("tp")
        self.C = math.gcd(heads_here, self.S)
        self.R = self.S // self.C
        s = lax.axis_index("sp")
        self.h = s // self.R
        self.q = s % self.R
        self.c = lax.axis_index("tp")

    def along_h(self, x, d):
        C, R = self.C, self.R
        return lax.ppermute(
            x, "sp", [(h * R + q, (h + d) % C * R + q) for h in range(C) for q in range(R)]
        )

    def along_q(self, x, d):
        C, R = self.C, self.R
        return lax.ppermute(
            x, "sp", [(h * R + q, h * R + (q + d) % R) for h in range(C) for q in range(R)]
        )

    def flip_q(self, x, d):
        C, R = self.C, self.R
        return lax.ppermute(
            x, "sp", [(h * R + q, h * R + (q ^ d)) for h in range(C) for q in range(R)]
        )

    def along_tp(self, x, d):
        T = self.T
        return lax.ppermute(x, "tp", [(c, (c + d) % T) for c in range(T)])

    def to_part(self, x, d):
        C, R = self.C, self.R
        return lax.ppermute(
            x, "sp", [(s, (s % C + d) % C * R + s // C) for s in range(self.S)]
        )

    def spread_heads(self, chunks_of):
        C = self.C
        got = [chunks_of(self.h)]
        for d in range(1, C):
            got.append(self.along_h(chunks_of((self.h + d) % C), d))
        rev = [got[(-k) % C] for k in range(C)]
        if C == 1:
            return rev[0][None]
        twice = jnp.stack(rev + rev)
        return lax.dynamic_slice_in_dim(twice, (C - self.h) % C, C, 0)

    def gather_parts(self, x):
        R = self.R
        n = x.shape[0]
        if R == 4 and n % 2 == 0:
            a = self.flip_q(x, 1)
            b = self.flip_q(x, 2)
            m = n // 2
            c = self.flip_q(a[:m], 2)
            d = self.flip_q(b[m:], 1)
            return [
                (self.q, 0, n, x),
                (self.q ^ 1, 0, n, a),
                (self.q ^ 2, 0, n, b),
                (self.q ^ 3, 0, m, c),
                (self.q ^ 3, m, n, d),
            ]
        if R <= 8:
            return [(self.q, 0, n, x)] + [
                ((self.q - d) % R, 0, n, self.along_q(x, d)) for d in range(1, R)
            ]
        groups = [[h * R + q for q in range(R)] for h in range(self.C)]
        g = lax.all_gather(x, "sp", axis=0, axis_index_groups=groups, tiled=False)
        return [(q, 0, n, g[q]) for q in range(R)]


def shards_general(
    tokens,
    norm_gain,
    conv_value_weight,
    conv_gate_weight,
    conv_kernel,
    conv_bias,
    channel_gain,
    query_weight,
    key_weight,
    value_weight,
    gate_weight,
    gate_offset,
    start_memory,
    start_norm,
    start_level,
    cell_gain,
    out_conv_weight,
    out_cell_weight,
):
    heads_here = start_level.shape[1]
    L = Layout(heads_here)
    S, T, C, R, h, q, c = L.S, L.T, L.C, L.R, L.h, L.q, L.c
    HL = heads_here // C
    B = tokens.shape[0]
    D = tokens.shape[1]
    N = B * C
    rows = D // S
    key_width = start_norm.shape[2]
    value_width = start_memory.shape[2]
    chan = conv_bias.shape[0] // C
    conv_all = conv_bias.shape[0] * T

    def mine(x, axis):
        n = x.shape[axis] // C
        return lax.dynamic_slice_in_dim(x, h * n, n, axis)

    features = tokens.astype(F32)
    normed = (
        features * lax.rsqrt(jnp.mean(features * features, axis=1, keepdims=True) + EPS) * norm_gain
    ).astype(BF16)
    normed = normed.reshape(B, C, R, rows).transpose(0, 2, 1, 3).reshape(B, D)
    half = D // T
    share = lax.dynamic_slice_in_dim(normed, c * half, half, 1)

    def columns(weights, line):
        return jnp.concatenate(
            [
                lax.dynamic_slice_in_dim(w, line * (w.shape[1] // C), w.shape[1] // C, 1)
                for w in weights
            ],
            axis=1,
        )

    def first(weights):
        got = L.spread_heads(lambda line: columns(weights, line))
        return got.reshape(C * rows, got.shape[2])

    conv_piece = first((conv_value_weight, conv_gate_weight))
    key_piece = first((key_weight,))
    value_piece = first((value_weight,))
    query_piece = first((query_weight,))

    got_tokens = [L.to_part(share, d) if C > 1 else share for d in range(C)]
    offsets = gate_offset.reshape(2, 2, C, HL, B)
    j_here = lax.axis_index("sp") % C
    got_offset = [
        L.to_part(pick(offsets, (j_here + d) % C, 2), d) if C > 1 else offsets[:, :, 0]
        for d in range(C)
    ]

    def in_order(got, axis):
        if C == 1:
            return got[0]
        rev = [got[(-k) % C] for k in range(C)]
        twice = jnp.concatenate(rev + rev, axis=axis)
        n = got[0].shape[axis]
        return lax.dynamic_slice_in_dim(twice, (C - h) % C * n, C * n, axis)

    share_all = in_order(got_tokens, 0)
    offset_all = in_order(got_offset, 3)
    others = [L.along_tp(share_all, d) for d in range(1, T)]
    parts = [share_all] + others
    rev = [parts[(-k) % T] for k in range(T)]
    hidden = lax.dynamic_slice_in_dim(
        jnp.concatenate(rev + rev, axis=1), (T - c) % T * half, D, 1
    )

    wide = C * rows

    def project(piece):
        total = None
        for part, lo, hi, w in L.gather_parts(piece):
            x = lax.dynamic_slice_in_dim(hidden, part * wide + lo, hi - lo, 1)
            y = dot(x, w)
            total = y if total is None else total + y
        return total

    conv_pre = project(conv_piece).astype(BF16)
    keys = project(key_piece).astype(BF16)
    values = project(value_piece).astype(BF16)
    queries = project(query_piece).astype(BF16)

    out_piece = L.spread_heads(
        lambda line: columns((out_conv_weight, out_cell_weight), line)
    ).reshape(C * rows, -1)
    out_rows = jnp.zeros((D, out_piece.shape[1]), BF16)
    for part, lo, hi, w in L.gather_parts(out_piece):
        out_rows = lax.dynamic_update_slice(out_rows, w, (part * wide + lo, 0))

    conv_value = conv_pre[:, :chan].astype(F32)
    conv_gate = conv_pre[:, chan:].astype(F32)
    gated = (conv_value * jax.nn.sigmoid(conv_gate)).astype(BF16)
    reach = conv_kernel.shape[0] // 2
    line_up = [(l * R + i, l * R + i + 1) for l in range(C) for i in range(R - 1)]
    before = lax.ppermute(gated[N - reach :], "sp", line_up)
    after = lax.ppermute(gated[:reach], "sp", [(b, a) for a, b in line_up])
    padded = jnp.concatenate([before, gated, after], axis=0).astype(F32)
    taps = mine(conv_kernel, 1)
    conv_sum = mine(conv_bias, 0) + sum(
        taps[k] * padded[k : k + N] for k in range(taps.shape[0])
    )
    stats = jnp.stack([jnp.sum(conv_sum, axis=1), jnp.sum(conv_sum * conv_sum, axis=1)])
    total = stats
    for d in range(C):
        for e in range(T):
            if d or e:
                total = total + lax.ppermute(
                    stats,
                    ("sp", "tp"),
                    [
                        ((l * R + p) * T + t, ((l + d) % C * R + p) * T + (t + e) % T)
                        for l in range(C)
                        for p in range(R)
                        for t in range(T)
                    ],
                )
    mean = total[0] / conv_all
    var = total[1] / conv_all - mean * mean
    conv_out = jax.nn.silu(
        (conv_sum - mean[:, None]) * lax.rsqrt(var + EPS)[:, None] * mine(channel_gain, 0)
    ).astype(BF16)

    groups = gate_weight.shape[1] // 4
    gates_w = gate_weight.reshape(C, R, rows, 4, groups)
    gates_w = lax.dynamic_slice_in_dim(gates_w, c * heads_here + h * HL, HL, 4)
    gates_w = gates_w.transpose(1, 0, 2, 3, 4).reshape(D, 4 * HL)
    gate_pre = dot(gates_w, hidden, ((0,), (1,))).reshape(2, 2, HL, N) + offset_all
    in_gate = gate_pre[:, 0]
    log_forget = jax.nn.log_sigmoid(gate_pre[:, 1])
    upto = (jnp.arange(N)[:, None] <= jnp.arange(N)[None, :]).astype(F32)
    forward_sum = jnp.dot(log_forget[0], upto, precision=lax.Precision.HIGHEST)
    backward_sum = jnp.dot(log_forget[1], upto.T, precision=lax.Precision.HIGHEST)
    sums = jnp.stack([forward_sum, backward_sum])
    passed = jnp.stack([forward_sum[:, -1], backward_sum[:, 0]])
    tail = passed[:, :, None] - sums + in_gate
    level = jnp.max(tail, axis=2)
    new_weight = jnp.exp(tail - level[:, :, None])
    my_memory = mine(start_memory, 1)
    my_norm = mine(start_norm, 1)
    my_level = mine(start_level, 1)
    step = jnp.arange(N)
    cells = []
    scale = key_width ** (-0.5)
    for i in range(HL):
        k = keys[:, i * key_width : (i + 1) * key_width] * jnp.asarray(scale, BF16)
        v = values[:, i * value_width : (i + 1) * value_width]
        qr = queries[:, i * key_width : (i + 1) * key_width]
        memories = []
        norms = []
        for d in range(2):
            w = new_weight[d, i]
            memories.append(dot((v.astype(F32) * w[:, None]).astype(BF16), k, ((0,), (0,))))
            norms.append(jnp.sum(w[:, None] * k.astype(F32), axis=0))
        memories = jnp.stack(memories).astype(BF16)
        smalls = jnp.concatenate(
            [jnp.stack(norms), level[:, i, None], passed[:, i, None]], axis=1
        )
        if R <= 8:
            got = []
            for d in range(1, R):
                back = jnp.where(q + d < R, 0, 1)
                got.append(
                    (L.along_q(pick(memories, back), d), L.along_q(pick(smalls, back), d))
                )
            get = lambda direction, dist: got[dist - 1 if direction == 0 else R - dist - 1]
        else:
            groups_q = [[l * R + p for p in range(R)] for l in range(C)]
            all_m = lax.all_gather(memories, "sp", axis=0, axis_index_groups=groups_q)
            all_s = lax.all_gather(smalls, "sp", axis=0, axis_index_groups=groups_q)

            def get(direction, dist):
                p = (q - dist) % R if direction == 0 else (q + dist) % R
                return pick(all_m, p)[direction], pick(all_s, p)[direction]

        scores = dot(qr, k, ((1,), (1,)))
        table_sum = None
        carried = None
        for direction in range(2):
            levels, mems, nrms = [], [], []
            decay = jnp.zeros((), F32)
            for dist in range(1, R):
                m, sm = get(direction, dist)
                there = q >= dist if direction == 0 else q + dist < R
                levels.append(jnp.where(there, sm[-2] + decay, LOW))
                mems.append(m)
                nrms.append(sm[:-2])
                decay = decay + jnp.where(there, sm[-1], 0.0)
            levels.append(my_level[direction, i] + decay)
            mems.append(my_memory[direction, i])
            nrms.append(my_norm[direction, i])
            run_level = levels[0]
            for lv in levels[1:]:
                run_level = jnp.maximum(run_level, lv)
            ws = [jnp.exp(lv - run_level) for lv in levels]
            memory = sum(w * m.astype(F32) for w, m in zip(ws, mems)).astype(BF16)
            norm = sum(w * n for w, n in zip(ws, nrms))
            f = sums[direction, i]
            g = in_gate[direction, i]
            mask = step[:, None] >= step[None, :] if direction == 0 else step[:, None] <= step[None, :]
            table = jnp.where(mask, f[:, None] + (g - f)[None, :], -jnp.inf)
            entry = f + run_level
            top = jnp.maximum(jnp.max(table, axis=1), entry)
            weights = scores * jnp.exp(table - top[:, None])
            ew = jnp.exp(entry - top)
            qn = jnp.sum(qr.astype(F32) * norm[None, :], axis=1)
            den = jnp.sum(weights, axis=1) + ew * qn
            inv = 1.0 / jnp.maximum(jnp.abs(den), 1.0)
            scaled = weights * inv[:, None]
            table_sum = scaled if table_sum is None else table_sum + scaled
            part = dot(qr, memory, ((1,), (1,))) * (ew * inv)[:, None]
            carried = part if carried is None else carried + part
        both = dot(table_sum.astype(BF16), v) + carried
        both = both * lax.rsqrt(jnp.mean(both * both, axis=1, keepdims=True) + EPS)
        gain = lax.dynamic_slice_in_dim(mine(cell_gain, 0), i * value_width, value_width, 0)
        cells.append((both * gain).astype(BF16))

    act = jnp.concatenate([conv_out] + cells, axis=1)
    strip = B // T
    act = act.reshape(C, T, strip, act.shape[1])

    def rows_for(t):
        x = pick(act, t, 1).reshape(C * strip, act.shape[3])
        return dot(x, out_rows, ((1,), (1,)))

    arrived = [L.along_tp(rows_for((c + d) % T).astype(BF16), d) for d in range(1, T)]
    own = rows_for(c)
    for a in arrived:
        own = own + a.astype(F32)
    blocks = own.astype(BF16).reshape(C, strip, D)

    if C == 1:
        final = blocks[0].astype(F32)
    elif C == R:
        got = [pick(blocks, q)]
        for d in range(1, R):
            got.append(L.along_q(pick(blocks, (q + d) % R), d))
        rev = [got[(-k) % R] for k in range(R)]
        by_part = jnp.stack(rev)
        final = pick(by_part, (h - q) % R).astype(F32)
        for d in range(1, C):
            final = final + L.along_h(pick(by_part, (h + d - q) % R), d).astype(F32)
    else:
        final = 0.0
        for d in range(C):
            perm = [(l * R + p, p * C + (l + d) % C) for l in range(C) for p in range(R)]
            final = final + lax.ppermute(pick(blocks, (h + d) % C), "sp", perm).astype(F32)
    final = final.astype(BF16).reshape(strip, R, C, rows).transpose(0, 2, 1, 3)
    return final.reshape(strip, D)


HIGHEST = lax.Precision.HIGHEST
NT = ((1,), (1,))
TN = ((0,), (0,))


def kernel(body, outs, pos, *args, scratch=(), limit=24 << 20, alias=None, part=None, far=False):
    specs, arrays = [], []
    for a in args:
        if isinstance(a, tuple) and a[1] is None:
            a = a[0]
            specs.append(pl.BlockSpec(memory_space=pl.ANY))
        elif isinstance(a, tuple):
            a, block, index = a
            specs.append(pl.BlockSpec(block, lambda i, p, index=index: index(p)))
        else:
            specs.append(pl.BlockSpec(a.shape, lambda i, p, k=a.ndim: (0,) * k))
        arrays.append(a)
    shapes = [pltpu.HBM(s, d) if far else jax.ShapeDtypeStruct(s, d) for s, d in outs]
    if part is None:
        part = [s for s, _ in outs]
    whole = [pl.BlockSpec(s, lambda i, p, k=len(s): (0,) * k) for s in part]
    many = len(shapes) > 1
    return pl.pallas_call(
        body,
        out_shape=shapes if many else shapes[0],
        grid_spec=pltpu.PrefetchScalarGridSpec(
            num_scalar_prefetch=1,
            grid=(1,),
            in_specs=specs,
            out_specs=whole if many else whole[0],
            scratch_shapes=scratch,
        ),
        compiler_params=pltpu.CompilerParams(vmem_limit_bytes=limit),
        input_output_aliases=alias or {},
    )(pos, *arrays)


def hbm(x):
    return pltpu.with_memory_space_constraint(x, pltpu.HBM)


def three(x):
    a = x.astype(BF16).astype(F32)
    b = (x - a).astype(BF16).astype(F32)
    return a, b, x - a - b


def turned_body(pos, *refs):
    outs = refs[-4:]
    each = (len(refs) - 4) // 4
    for d, out in enumerate(outs):
        at = 0
        for w in refs[d * each : (d + 1) * each]:
            out[:, at : at + w.shape[1]] = w[...]
            at += w.shape[1]


def straight_body(pos, *refs):
    out = refs[-1]
    for l in range(out.shape[0]):
        at = 0
        for w in refs[:-1]:
            m = w.shape[1] // out.shape[0]
            out[l, :, at : at + m] = w[:, l * m : (l + 1) * m]
            at += m


def stack_body(pos, g0, g1, g2, g3, out):
    for d, g in enumerate((g0, g1, g2, g3)):
        out[lax.rem(pos[0] - d + 4, 4)] = g[...]


def norm_body(pos, tok, gain, off, share):
    C, R = 4, 4
    B, D = tok.shape
    rows = D // (C * R)
    x = tok[...].astype(F32)
    y = x * lax.rsqrt(jnp.mean(x * x, axis=1, keepdims=True) + EPS) * gain[...]
    y = y.astype(BF16)
    halves = []
    for t in range(2):
        halves.append(
            jnp.concatenate(
                [
                    y[:, (hh * R + qq) * rows : (hh * R + qq + 1) * rows]
                    for qq in (2 * t, 2 * t + 1)
                    for hh in range(C)
                ],
                axis=1,
            )
        )
    share[0:B, :] = jnp.where(pos[2] == 0, halves[0], halves[1])
    o = jnp.concatenate([off[k] for k in range(4)], axis=1)
    a, b, c = three(o)
    extra = jnp.concatenate(
        [jnp.concatenate([a, b], axis=1), jnp.concatenate([c, jnp.zeros_like(c)], axis=1)], axis=0
    )
    extra = jnp.concatenate([extra, jnp.zeros_like(extra)], axis=0)
    share[B : B + 16, :] = extra.astype(BF16)


def arrange_body(pos, g0, g1, g2, g3, own, offs):
    h = pos[0]
    B = own.shape[1]
    for d, g in enumerate((g0, g1, g2, g3)):
        j = lax.rem(h - d + 4, 4)
        own[j] = g[0:B, :]
        e = g[B : B + 16, :].astype(F32)
        row = lax.broadcasted_iota(jnp.int32, e.shape, 0)
        ab = jnp.sum(jnp.where(row == h, e, 0.0), axis=0, keepdims=True)
        cc = jnp.sum(jnp.where(row == h + 4, e, 0.0), axis=0, keepdims=True)
        n = ab.shape[1] // 2
        o = ab[:, :n] + ab[:, n:] + cc[:, :n]
        for k in range(4):
            offs[j, k : k + 1, :] = o[:, k * B : (k + 1) * B]


def fill_hidden(pos, own, other, hid):
    c = pos[2]
    n = own.shape[1] // 2
    for i in range(2):
        hid[2 * c + i] = own[:, i * n : (i + 1) * n]
        hid[2 - 2 * c + i] = other[:, i * n : (i + 1) * n]


def projected(pos, hid, pieces):
    q = pos[1]
    y = None
    for i, w in enumerate(pieces):
        t = dot(hid[q ^ i], w[...])
        y = t if y is None else y + t
    return y


def state_body(
    pos, own, other, a0, a1, a2, a3, b0, b1, b2, b3, gw, offs,
    k_out, v_out, g_out, gated, msg, hid, pre_t
):
    h, q, c = pos[0], pos[1], pos[2]
    fill_hidden(pos, own, other, hid)
    R, N, _ = hid.shape
    kw = k_out.shape[1]
    n = gated.shape[1]
    y = projected(pos, hid, (a0, a1, a2, a3))
    k = (y[:, :kw].astype(BF16).astype(F32) * (kw ** (-0.5))).astype(BF16)
    k_out[...] = k
    a = y[:, kw : kw + n].astype(BF16).astype(F32)
    g = y[:, kw + n :].astype(BF16).astype(F32)
    z = (a * jax.nn.sigmoid(g)).astype(BF16)
    gated[...] = z
    edges = jnp.concatenate([z[0:16, :], z[N - 16 :, :]], axis=1)
    rows = gw.shape[1] // 16
    pre = None
    for p in range(R):
        w = jnp.concatenate(
            [gw[:, (l * R + p) * rows : (l * R + p + 1) * rows] for l in range(4)], axis=1
        )
        t = dot(w, hid[p], NT)
        pre = t if pre is None else pre + t
    pre_t[...] = pre
    heads = gw.shape[0] // 4
    at = c * 4 + h
    pre = jnp.concatenate([pre_t[pl.ds(i * heads + at, 1), :] for i in range(4)], axis=0)
    off = jnp.concatenate([offs[j] for j in range(4)], axis=1)
    pre = pre + off
    lf = jnp.minimum(pre, 0.0) - jnp.log1p(jnp.exp(-jnp.abs(pre)))
    lf8 = jnp.concatenate([lf, lf], axis=0)
    ri = lax.broadcasted_iota(jnp.int32, (N, N), 0)
    ci = lax.broadcasted_iota(jnp.int32, (N, N), 1)
    up = jnp.where(ri <= ci, 1.0, 0.0).astype(BF16)
    down = jnp.where(ri >= ci, 1.0, 0.0).astype(BF16)
    f, b = None, None
    for t in three(lf8):
        t = t.astype(BF16)
        f1, b1_ = dot(t, up), dot(t, down)
        f = f1 if f is None else f + f1
        b = b1_ if b is None else b + b1_
    f, b = f[1:2], b[3:4]
    inf, inb = pre[0:1], pre[2:3]
    pf, pb = f[:, N - 1 : N], b[:, 0:1]
    tf, tb = pf - f + inf, pb - b + inb
    lvf, lvb = jnp.max(tf, axis=1, keepdims=True), jnp.max(tb, axis=1, keepdims=True)
    wf, wb = jnp.exp(tf - lvf), jnp.exp(tb - lvb)
    zero = jnp.zeros_like(f)
    g_out[...] = jnp.concatenate([f, b, inf - f, inb - b, zero, zero, zero, zero], axis=0)
    w8 = jnp.concatenate([wf, wb, zero, zero, zero, zero, zero, zero], axis=0)
    wt = w8.T
    nn = None
    for t in three(w8):
        t = dot(t.astype(BF16), k)
        nn = t if nn is None else nn + t
    v = projected(pos, hid, (b0, b1, b2, b3)).astype(BF16)
    v_out[...] = v
    v32 = v.astype(F32)
    mf = dot((v32 * wt[:, 0:1]).astype(BF16), k, TN).astype(BF16)
    mb = dot((v32 * wt[:, 1:2]).astype(BF16), k, TN).astype(BF16)

    def small(n1, lv, ps):
        wide_ = lambda x: jnp.broadcast_to(x, n1.shape)
        r = list(three(n1)) + [wide_(x) for x in three(lv)] + [wide_(x) for x in three(ps)]
        return jnp.concatenate(r + [jnp.zeros((7, n1.shape[1]), F32)], axis=0).astype(BF16)

    sf, sb = small(nn[0:1], lvf, pf), small(nn[1:2], lvb, pb)
    vw = mf.shape[0]
    for p in range(R):
        msg[p, vw + 16 : vw + 32, 0 : 2 * n] = edges

        @pl.when(p > q)
        def _():
            msg[p, 0:vw, :] = mf
            msg[p, vw : vw + 16, :] = sf

        @pl.when(p <= q)
        def _():
            msg[p, 0:vw, :] = mb
            msg[p, vw : vw + 16, :] = sb


def conv_body(pos, gated, msg, taps, bias, conv, stats, pad):
    q = pos[1]
    N, n = gated.shape
    K = taps.shape[0]
    at = msg.shape[1] - 16
    last = msg.shape[0] - 1
    left = msg[jnp.maximum(q - 1, 0), at : at + 16, n : 2 * n].astype(F32)
    right = msg[jnp.minimum(q + 1, last), at : at + 16, 0:n].astype(F32)
    pad[0:16, :] = jnp.where(q > 0, left, 0.0)
    pad[16 : 16 + N, :] = gated[...].astype(F32)
    pad[16 + N : 32 + N, :] = jnp.where(q < last, right, 0.0)
    lo = 16 - K // 2
    step = 64
    for r in range(0, N, step):
        acc = jnp.broadcast_to(bias[...], (step, n))
        for k in range(K):
            acc = acc + taps[k : k + 1, :] * pad[lo + k + r : lo + k + r + step, :]
        conv[r : r + step, :] = acc
    x = conv[...]
    ones = jnp.ones((8, n), F32)
    s1 = lax.dot_general(ones, x, (NT, ((), ())), precision=HIGHEST, preferred_element_type=F32)
    s2 = lax.dot_general(ones, x * x, (NT, ((), ())), precision=HIGHEST, preferred_element_type=F32)
    row = lax.broadcasted_iota(jnp.int32, s1.shape, 0)
    both = jnp.where(row == 0, s1, s2)
    for i in range(stats.shape[0]):
        stats[i] = both


def cell_body(
    pos, own, other, c0, c1, c2, c3, k, v, g, msg, mem0, nrm0, lev0, gain, act, hid, qs
):
    h, q = pos[0], pos[1]
    fill_hidden(pos, own, other, hid)
    qs[...] = projected(pos, hid, (c0, c1, c2, c3)).astype(BF16)
    N = qs.shape[0]
    vw = v.shape[1]
    lv, ps, nr = [], [], []
    for p in range(4):
        e = msg[p, vw : vw + 16, :].astype(F32)
        nr.append(e[0:1] + e[1:2] + e[2:3])
        lv.append((e[3:4] + e[4:5] + e[5:6])[:, 0:1])
        ps.append((e[6:7] + e[7:8] + e[8:9])[:, 0:1])
    mems, nrms, runs = [], [], []
    for d in range(2):
        def ok(p):
            return p < q if d == 0 else p > q

        lvs = []
        for p in range(4):
            between = range(p + 1, 4) if d == 0 else range(0, p)
            x = lv[p]
            for m in between:
                x = x + jnp.where(ok(m), ps[m], 0.0)
            lvs.append(jnp.where(ok(p), x, LOW))
        x = lev0[d : d + 1, :]
        x = jnp.where(lax.broadcasted_iota(jnp.int32, x.shape, 1) == h, x, 0.0)
        x = jnp.sum(x, axis=1, keepdims=True)
        for m in range(4):
            x = x + jnp.where(ok(m), ps[m], 0.0)
        lvs.append(x)
        run = lvs[0]
        for y in lvs[1:]:
            run = jnp.maximum(run, y)
        ws = [jnp.exp(y - run) for y in lvs]
        mm = ws[4] * mem0[d, 0]
        nm = ws[4] * nrm0[d, pl.ds(h, 1), :]
        for p in range(4):
            mm = mm + ws[p] * msg[p, 0:vw, :].astype(F32)
            nm = nm + ws[p] * nr[p]
        mems.append(mm.astype(BF16))
        nrms.append(nm)
        runs.append(run)
    gt = g[...].T
    gn = gain[pl.ds(h, 1), :]
    blk = N // 4
    for j in range(4):
        r0 = j * blk
        qb = qs[r0 : r0 + blk, :]
        q32 = qb.astype(F32)
        scores = dot(qb, k[...], NT)
        ri = lax.broadcasted_iota(jnp.int32, (blk, N), 0) + r0
        ci = lax.broadcasted_iota(jnp.int32, (blk, N), 1)
        total, both = None, None
        for d in range(2):
            fc = gt[r0 : r0 + blk, d : d + 1]
            mask = ri >= ci if d == 0 else ri <= ci
            table = jnp.where(mask, fc + g[2 + d : 3 + d, :], -jnp.inf)
            entry = fc + runs[d]
            top = jnp.maximum(jnp.max(table, axis=1, keepdims=True), entry)
            w = scores * jnp.exp(table - top)
            ew = jnp.exp(entry - top)
            den = jnp.sum(w, axis=1, keepdims=True)
            den = den + ew * jnp.sum(q32 * nrms[d], axis=1, keepdims=True)
            inv = 1.0 / jnp.maximum(jnp.abs(den), 1.0)
            w = w * inv
            total = w if total is None else total + w
            part = dot(qb, mems[d], NT) * (ew * inv)
            both = part if both is None else both + part
        both = both + dot(total.astype(BF16), v[...])
        both = both * lax.rsqrt(jnp.mean(both * both, axis=1, keepdims=True) + EPS) * gn
        act[r0 : r0 + blk, act.shape[1] - vw :] = both.astype(BF16)


def join_body(pos, conv, stats, gain, held, act):
    n = conv.shape[1]
    st = stats[0]
    for i in range(1, stats.shape[0]):
        st = st + stats[i]
    width = n * stats.shape[0]
    mean = st[0:1] / width
    var = st[1:2] / width - mean * mean
    mv = jnp.concatenate([mean, lax.rsqrt(var + EPS)] + [jnp.zeros_like(mean)] * 6, axis=0).T
    x = (conv[...] - mv[:, 0:1]) * mv[:, 1:2] * gain[...]
    act[...] = (x * jax.nn.sigmoid(x)).astype(BF16)


def out_body(pos, act, w0, w1, give, keep):
    c = pos[2]
    half = act.shape[1] // 2

    def rows_of(t):
        at = pl.multiple_of(t * half, half)
        return jnp.concatenate([act[p, pl.ds(at, half), :] for p in range(act.shape[0])], axis=0)

    x, y = rows_of(1 - c), rows_of(c)
    m = w0.shape[0]
    for i, w in enumerate((w0, w1)):
        give[:, i * m : (i + 1) * m] = dot(x, w[...], NT).astype(BF16)
    for i, w in enumerate((w0, w1)):
        keep[:, i * m : (i + 1) * m] = dot(y, w[...], NT)


def add_body(pos, keep, got, *outs):
    n = outs[0].shape[0]
    for d, out in enumerate(outs):
        at = pl.multiple_of(lax.rem(pos[0] + d, len(outs)) * n, n)
        out[...] = (keep[pl.ds(at, n), :] + got[pl.ds(at, n), :].astype(F32)).astype(BF16)


def last_body(pos, *refs):
    out, tiles = refs[-2:]
    q = pos[1]
    each = (len(refs) - 2) // 2
    for y in range(2):
        x = None
        for r in refs[y * each : (y + 1) * each]:
            x = r[...].astype(F32) if x is None else x + r[...].astype(F32)
        rows = x.shape[1] // 8
        for i in range(2):
            for l in range(4):
                at = i * 4 + l
                tiles[l * 4 + (q ^ (2 * y + i))] = x[:, at * rows : (at + 1) * rows]
    out[...] = jnp.concatenate([tiles[i] for i in range(16)], axis=1).astype(BF16)


def shards(
    tokens,
    norm_gain,
    conv_value_weight,
    conv_gate_weight,
    conv_kernel,
    conv_bias,
    channel_gain,
    query_weight,
    key_weight,
    value_weight,
    gate_weight,
    gate_offset,
    start_memory,
    start_norm,
    start_level,
    cell_gain,
    out_conv_weight,
    out_cell_weight,
):
    heads_here = start_level.shape[1]
    L = Layout(heads_here)
    S, T, C, R, h, q, c = L.S, L.T, L.C, L.R, L.h, L.q, L.c
    B, D = tokens.shape
    N = B * C
    rows = D // S
    kw = start_norm.shape[2]
    vw = start_memory.shape[2]
    n = conv_bias.shape[0] // C
    fits = C == R == 4 and T == 2 and heads_here == C and B % 128 == 0 and rows % 128 == 0
    fits = fits and n % 128 == 0 and kw % 128 == 0 and vw % 128 == 0 and conv_kernel.shape[0] <= 31
    fits = fits and 2 * n <= kw
    if not fits:
        return shards_general(
            tokens,
            norm_gain,
            conv_value_weight,
            conv_gate_weight,
            conv_kernel,
            conv_bias,
            channel_gain,
            query_weight,
            key_weight,
            value_weight,
            gate_weight,
            gate_offset,
            start_memory,
            start_norm,
            start_level,
            cell_gain,
            out_conv_weight,
            out_cell_weight,
        )
    pos = jnp.stack([h, q, c, jnp.zeros_like(h)]).astype(jnp.int32)
    lines = [[l * R + p for l in range(C)] for p in range(R)]
    planes = [[l * R + p for p in range(R)] for l in range(C)]

    def swap(x, groups, axes="sp"):
        return lax.all_to_all(x, axes, 0, 0, axis_index_groups=groups, tiled=True)

    def flip(x, d):
        return L.flip_q(x, d)

    def at_col(x):
        m = x.shape[1] // C
        return (hbm(x), (x.shape[0], m), lambda p: (0, p[0]))

    wide = C * rows

    def turned(weights):
        blocks = [
            (hbm(w), (rows, w.shape[1] // C), lambda p, d=d: (0, lax.rem(p[0] + d, C)))
            for d in range(C)
            for w in weights
        ]
        width = sum(w.shape[1] for w in weights) // C
        return kernel(turned_body, [((rows, width), BF16)] * C, pos, *blocks)

    def straight(weights):
        width = sum(w.shape[1] for w in weights) // C
        return kernel(straight_body, [((C, rows, width), BF16)], pos, *map(hbm, weights))

    def cross(turn):
        got = [turn[0]]
        for d in range(1, C):
            got.append(L.along_h(turn[d], d))
        shape = (C, rows, turn[0].shape[1])
        out = kernel(stack_body, [(shape, BF16)], pos, *got)
        return out.reshape(wide, -1)

    z_a = cross(turned((key_weight, conv_value_weight, conv_gate_weight)))
    z_b = swap(straight((value_weight,)), lines).reshape(wide, -1)
    share = kernel(
        norm_body,
        [((B + 16, D // 2), BF16)],
        pos,
        hbm(tokens),
        norm_gain.reshape(1, D),
        gate_offset.reshape(4, heads_here, B),
    )
    got = []
    for d in range(C):
        got.append(L.to_part(share, d))
    z_q = cross(turned((query_weight,)))
    z_o = cross(turned((out_conv_weight, out_cell_weight)))

    a1, a2 = flip(z_a, 1), flip(z_a, 2)
    b1, b2 = flip(z_b, 1), flip(z_b, 2)
    a3 = flip(a1, 2)
    b3 = flip(b2, 1)
    q1, q2 = flip(z_q, 1), flip(z_q, 2)
    q3 = flip(q1, 2)
    o1, o2 = flip(z_o, 1), flip(z_o, 2)
    o3 = flip(o1, 2)

    own, offs = kernel(arrange_body, [((C, B, D // 2), BF16), ((C, 4, B), F32)], pos, *got)
    own = own.reshape(N, D // 2)
    other = L.along_tp(own, 1)
    hid = pltpu.VMEM((R, N, wide), BF16)
    keys, values, gates, gated, msg = kernel(
        state_body,
        [
            ((N, kw), BF16),
            ((N, vw), BF16),
            ((8, N), F32),
            ((N, n), BF16),
            ((R, vw + 32, kw), BF16),
        ],
        pos,
        own,
        other,
        z_a,
        a1,
        a2,
        a3,
        z_b,
        b1,
        b2,
        b3,
        gate_weight.T,
        offs,
        scratch=[hid, pltpu.VMEM((gate_weight.shape[1], N), F32)],
        far=True,
    )
    msg = swap(msg, planes)
    conv, stats = kernel(
        conv_body,
        [((N, n), F32), ((C * T, 8, N), F32)],
        pos,
        hbm(gated),
        msg,
        at_col(conv_kernel),
        at_col(conv_bias.reshape(1, C * n)),
        scratch=[pltpu.VMEM((N + 32, n), F32)],
        far=True,
    )
    stats = swap(
        stats,
        [[(l * R + p) * T + t for l in range(C) for t in range(T)] for p in range(R)],
        ("sp", "tp"),
    )
    act = kernel(
        cell_body,
        [((N, n + vw), BF16)],
        pos,
        own,
        other,
        z_q,
        q1,
        q2,
        q3,
        hbm(keys),
        hbm(values),
        hbm(gates),
        msg,
        (hbm(start_memory), (2, 1, vw, kw), lambda p: (0, p[0], 0, 0)),
        hbm(start_norm),
        hbm(start_level),
        hbm(cell_gain.reshape(C, vw)),
        scratch=[hid, pltpu.VMEM((N, kw), BF16)],
    )
    act = kernel(
        join_body,
        [((N, n + vw), BF16)],
        pos,
        hbm(conv),
        stats,
        at_col(channel_gain.reshape(1, C * n)),
        (act, None),
        alias={4: 0},
        part=[(N, n)],
    )
    act = swap(act.reshape(C, B, n + vw), planes)
    ends = []
    for w0, w1 in ((z_o, o1), (o2, o3)):
        give, keep = kernel(
            out_body, [((N // 2, 2 * wide), BF16), ((N // 2, 2 * wide), F32)], pos, act, w0, w1
        )
        give = L.along_tp(give, 1)
        blocks = kernel(add_body, [((B // T, 2 * wide), BF16)] * C, pos, keep, give)
        ends.append(blocks[0])
        for d in range(1, C):
            ends.append(L.along_h(blocks[d], d))
    return kernel(
        last_body, [((B // T, D), BF16)], pos, *ends, scratch=[pltpu.VMEM((16, B // T, rows), F32)]
    )


def solution(mesh):
    in_specs = (
        P("sp", None),
        P(),
        P("sp", "tp"),
        P("sp", "tp"),
        P(None, "tp"),
        P("tp"),
        P("tp"),
        P("sp", "tp"),
        P("sp", "tp"),
        P("sp", "tp"),
        P(),
        P(None, None, "tp", "sp"),
        P(None, "tp", None, None),
        P(None, "tp", None),
        P(None, "tp"),
        P("tp"),
        P("sp", "tp"),
        P("sp", "tp"),
    )
    out_specs = P(("sp", "tp"), None)
    return jax.shard_map(shards, mesh=mesh, in_specs=in_specs, out_specs=out_specs, check_vma=False)
```

```python
import math

import jax
import jax.numpy as jnp
from jax import lax
from jax.experimental import pallas as pl
from jax.experimental.pallas import tpu as pltpu
from jax.sharding import PartitionSpec as P


EPS = 1e-06
LOW = -1e30
F32 = jnp.float32
BF16 = jnp.bfloat16


def dot(a, b, dims=((1,), (0,))):
    return lax.dot_general(a, b, (dims, ((), ())), preferred_element_type=F32)


def pick(stack, index, axis=0):
    return lax.dynamic_index_in_dim(stack, index, axis, keepdims=False)


class Layout:
    def __init__(self, heads_here):
        self.S = lax.axis_size("sp")
        self.T = lax.axis_size("tp")
        self.C = math.gcd(heads_here, self.S)
        self.R = self.S // self.C
        s = lax.axis_index("sp")
        self.h = s // self.R
        self.q = s % self.R
        self.c = lax.axis_index("tp")

    def along_h(self, x, d):
        C, R = self.C, self.R
        return lax.ppermute(
            x, "sp", [(h * R + q, (h + d) % C * R + q) for h in range(C) for q in range(R)]
        )

    def along_q(self, x, d):
        C, R = self.C, self.R
        return lax.ppermute(
            x, "sp", [(h * R + q, h * R + (q + d) % R) for h in range(C) for q in range(R)]
        )

    def flip_q(self, x, d):
        C, R = self.C, self.R
        return lax.ppermute(
            x, "sp", [(h * R + q, h * R + (q ^ d)) for h in range(C) for q in range(R)]
        )

    def along_tp(self, x, d):
        T = self.T
        return lax.ppermute(x, "tp", [(c, (c + d) % T) for c in range(T)])

    def to_part(self, x, d):
        C, R = self.C, self.R
        return lax.ppermute(
            x, "sp", [(s, (s % C + d) % C * R + s // C) for s in range(self.S)]
        )

    def spread_heads(self, chunks_of):
        C = self.C
        got = [chunks_of(self.h)]
        for d in range(1, C):
            got.append(self.along_h(chunks_of((self.h + d) % C), d))
        rev = [got[(-k) % C] for k in range(C)]
        if C == 1:
            return rev[0][None]
        twice = jnp.stack(rev + rev)
        return lax.dynamic_slice_in_dim(twice, (C - self.h) % C, C, 0)

    def gather_parts(self, x):
        R = self.R
        n = x.shape[0]
        if R == 4 and n % 2 == 0:
            a = self.flip_q(x, 1)
            b = self.flip_q(x, 2)
            m = n // 2
            c = self.flip_q(a[:m], 2)
            d = self.flip_q(b[m:], 1)
            return [
                (self.q, 0, n, x),
                (self.q ^ 1, 0, n, a),
                (self.q ^ 2, 0, n, b),
                (self.q ^ 3, 0, m, c),
                (self.q ^ 3, m, n, d),
            ]
        if R <= 8:
            return [(self.q, 0, n, x)] + [
                ((self.q - d) % R, 0, n, self.along_q(x, d)) for d in range(1, R)
            ]
        groups = [[h * R + q for q in range(R)] for h in range(self.C)]
        g = lax.all_gather(x, "sp", axis=0, axis_index_groups=groups, tiled=False)
        return [(q, 0, n, g[q]) for q in range(R)]


def shards_general(
    tokens,
    norm_gain,
    conv_value_weight,
    conv_gate_weight,
    conv_kernel,
    conv_bias,
    channel_gain,
    query_weight,
    key_weight,
    value_weight,
    gate_weight,
    gate_offset,
    start_memory,
    start_norm,
    start_level,
    cell_gain,
    out_conv_weight,
    out_cell_weight,
):
    heads_here = start_level.shape[1]
    L = Layout(heads_here)
    S, T, C, R, h, q, c = L.S, L.T, L.C, L.R, L.h, L.q, L.c
    HL = heads_here // C
    B = tokens.shape[0]
    D = tokens.shape[1]
    N = B * C
    rows = D // S
    key_width = start_norm.shape[2]
    value_width = start_memory.shape[2]
    chan = conv_bias.shape[0] // C
    conv_all = conv_bias.shape[0] * T

    def mine(x, axis):
        n = x.shape[axis] // C
        return lax.dynamic_slice_in_dim(x, h * n, n, axis)

    features = tokens.astype(F32)
    normed = (
        features * lax.rsqrt(jnp.mean(features * features, axis=1, keepdims=True) + EPS) * norm_gain
    ).astype(BF16)
    normed = normed.reshape(B, C, R, rows).transpose(0, 2, 1, 3).reshape(B, D)
    half = D // T
    share = lax.dynamic_slice_in_dim(normed, c * half, half, 1)

    def columns(weights, line):
        return jnp.concatenate(
            [
                lax.dynamic_slice_in_dim(w, line * (w.shape[1] // C), w.shape[1] // C, 1)
                for w in weights
            ],
            axis=1,
        )

    def first(weights):
        got = L.spread_heads(lambda line: columns(weights, line))
        return got.reshape(C * rows, got.shape[2])

    conv_piece = first((conv_value_weight, conv_gate_weight))
    key_piece = first((key_weight,))
    value_piece = first((value_weight,))
    query_piece = first((query_weight,))

    got_tokens = [L.to_part(share, d) if C > 1 else share for d in range(C)]
    offsets = gate_offset.reshape(2, 2, C, HL, B)
    j_here = lax.axis_index("sp") % C
    got_offset = [
        L.to_part(pick(offsets, (j_here + d) % C, 2), d) if C > 1 else offsets[:, :, 0]
        for d in range(C)
    ]

    def in_order(got, axis):
        if C == 1:
            return got[0]
        rev = [got[(-k) % C] for k in range(C)]
        twice = jnp.concatenate(rev + rev, axis=axis)
        n = got[0].shape[axis]
        return lax.dynamic_slice_in_dim(twice, (C - h) % C * n, C * n, axis)

    share_all = in_order(got_tokens, 0)
    offset_all = in_order(got_offset, 3)
    others = [L.along_tp(share_all, d) for d in range(1, T)]
    parts = [share_all] + others
    rev = [parts[(-k) % T] for k in range(T)]
    hidden = lax.dynamic_slice_in_dim(
        jnp.concatenate(rev + rev, axis=1), (T - c) % T * half, D, 1
    )

    wide = C * rows

    def project(piece):
        total = None
        for part, lo, hi, w in L.gather_parts(piece):
            x = lax.dynamic_slice_in_dim(hidden, part * wide + lo, hi - lo, 1)
            y = dot(x, w)
            total = y if total is None else total + y
        return total

    conv_pre = project(conv_piece).astype(BF16)
    keys = project(key_piece).astype(BF16)
    values = project(value_piece).astype(BF16)
    queries = project(query_piece).astype(BF16)

    out_piece = L.spread_heads(
        lambda line: columns((out_conv_weight, out_cell_weight), line)
    ).reshape(C * rows, -1)
    out_rows = jnp.zeros((D, out_piece.shape[1]), BF16)
    for part, lo, hi, w in L.gather_parts(out_piece):
        out_rows = lax.dynamic_update_slice(out_rows, w, (part * wide + lo, 0))

    conv_value = conv_pre[:, :chan].astype(F32)
    conv_gate = conv_pre[:, chan:].astype(F32)
    gated = (conv_value * jax.nn.sigmoid(conv_gate)).astype(BF16)
    reach = conv_kernel.shape[0] // 2
    line_up = [(l * R + i, l * R + i + 1) for l in range(C) for i in range(R - 1)]
    before = lax.ppermute(gated[N - reach :], "sp", line_up)
    after = lax.ppermute(gated[:reach], "sp", [(b, a) for a, b in line_up])
    padded = jnp.concatenate([before, gated, after], axis=0).astype(F32)
    taps = mine(conv_kernel, 1)
    conv_sum = mine(conv_bias, 0) + sum(
        taps[k] * padded[k : k + N] for k in range(taps.shape[0])
    )
    stats = jnp.stack([jnp.sum(conv_sum, axis=1), jnp.sum(conv_sum * conv_sum, axis=1)])
    total = stats
    for d in range(C):
        for e in range(T):
            if d or e:
                total = total + lax.ppermute(
                    stats,
                    ("sp", "tp"),
                    [
                        ((l * R + p) * T + t, ((l + d) % C * R + p) * T + (t + e) % T)
                        for l in range(C)
                        for p in range(R)
                        for t in range(T)
                    ],
                )
    mean = total[0] / conv_all
    var = total[1] / conv_all - mean * mean
    conv_out = jax.nn.silu(
        (conv_sum - mean[:, None]) * lax.rsqrt(var + EPS)[:, None] * mine(channel_gain, 0)
    ).astype(BF16)

    groups = gate_weight.shape[1] // 4
    gates_w = gate_weight.reshape(C, R, rows, 4, groups)
    gates_w = lax.dynamic_slice_in_dim(gates_w, c * heads_here + h * HL, HL, 4)
    gates_w = gates_w.transpose(1, 0, 2, 3, 4).reshape(D, 4 * HL)
    gate_pre = dot(gates_w, hidden, ((0,), (1,))).reshape(2, 2, HL, N) + offset_all
    in_gate = gate_pre[:, 0]
    log_forget = jax.nn.log_sigmoid(gate_pre[:, 1])
    upto = (jnp.arange(N)[:, None] <= jnp.arange(N)[None, :]).astype(F32)
    forward_sum = jnp.dot(log_forget[0], upto, precision=lax.Precision.HIGHEST)
    backward_sum = jnp.dot(log_forget[1], upto.T, precision=lax.Precision.HIGHEST)
    sums = jnp.stack([forward_sum, backward_sum])
    passed = jnp.stack([forward_sum[:, -1], backward_sum[:, 0]])
    tail = passed[:, :, None] - sums + in_gate
    level = jnp.max(tail, axis=2)
    new_weight = jnp.exp(tail - level[:, :, None])
    my_memory = mine(start_memory, 1)
    my_norm = mine(start_norm, 1)
    my_level = mine(start_level, 1)
    step = jnp.arange(N)
    cells = []
    scale = key_width ** (-0.5)
    for i in range(HL):
        k = keys[:, i * key_width : (i + 1) * key_width] * jnp.asarray(scale, BF16)
        v = values[:, i * value_width : (i + 1) * value_width]
        qr = queries[:, i * key_width : (i + 1) * key_width]
        memories = []
        norms = []
        for d in range(2):
            w = new_weight[d, i]
            memories.append(dot((v.astype(F32) * w[:, None]).astype(BF16), k, ((0,), (0,))))
            norms.append(jnp.sum(w[:, None] * k.astype(F32), axis=0))
        memories = jnp.stack(memories).astype(BF16)
        smalls = jnp.concatenate(
            [jnp.stack(norms), level[:, i, None], passed[:, i, None]], axis=1
        )
        if R <= 8:
            got = []
            for d in range(1, R):
                back = jnp.where(q + d < R, 0, 1)
                got.append(
                    (L.along_q(pick(memories, back), d), L.along_q(pick(smalls, back), d))
                )
            get = lambda direction, dist: got[dist - 1 if direction == 0 else R - dist - 1]
        else:
            groups_q = [[l * R + p for p in range(R)] for l in range(C)]
            all_m = lax.all_gather(memories, "sp", axis=0, axis_index_groups=groups_q)
            all_s = lax.all_gather(smalls, "sp", axis=0, axis_index_groups=groups_q)

            def get(direction, dist):
                p = (q - dist) % R if direction == 0 else (q + dist) % R
                return pick(all_m, p)[direction], pick(all_s, p)[direction]

        scores = dot(qr, k, ((1,), (1,)))
        table_sum = None
        carried = None
        for direction in range(2):
            levels, mems, nrms = [], [], []
            decay = jnp.zeros((), F32)
            for dist in range(1, R):
                m, sm = get(direction, dist)
                there = q >= dist if direction == 0 else q + dist < R
                levels.append(jnp.where(there, sm[-2] + decay, LOW))
                mems.append(m)
                nrms.append(sm[:-2])
                decay = decay + jnp.where(there, sm[-1], 0.0)
            levels.append(my_level[direction, i] + decay)
            mems.append(my_memory[direction, i])
            nrms.append(my_norm[direction, i])
            run_level = levels[0]
            for lv in levels[1:]:
                run_level = jnp.maximum(run_level, lv)
            ws = [jnp.exp(lv - run_level) for lv in levels]
            memory = sum(w * m.astype(F32) for w, m in zip(ws, mems)).astype(BF16)
            norm = sum(w * n for w, n in zip(ws, nrms))
            f = sums[direction, i]
            g = in_gate[direction, i]
            mask = step[:, None] >= step[None, :] if direction == 0 else step[:, None] <= step[None, :]
            table = jnp.where(mask, f[:, None] + (g - f)[None, :], -jnp.inf)
            entry = f + run_level
            top = jnp.maximum(jnp.max(table, axis=1), entry)
            weights = scores * jnp.exp(table - top[:, None])
            ew = jnp.exp(entry - top)
            qn = jnp.sum(qr.astype(F32) * norm[None, :], axis=1)
            den = jnp.sum(weights, axis=1) + ew * qn
            inv = 1.0 / jnp.maximum(jnp.abs(den), 1.0)
            scaled = weights * inv[:, None]
            table_sum = scaled if table_sum is None else table_sum + scaled
            part = dot(qr, memory, ((1,), (1,))) * (ew * inv)[:, None]
            carried = part if carried is None else carried + part
        both = dot(table_sum.astype(BF16), v) + carried
        both = both * lax.rsqrt(jnp.mean(both * both, axis=1, keepdims=True) + EPS)
        gain = lax.dynamic_slice_in_dim(mine(cell_gain, 0), i * value_width, value_width, 0)
        cells.append((both * gain).astype(BF16))

    act = jnp.concatenate([conv_out] + cells, axis=1)
    strip = B // T
    act = act.reshape(C, T, strip, act.shape[1])

    def rows_for(t):
        x = pick(act, t, 1).reshape(C * strip, act.shape[3])
        return dot(x, out_rows, ((1,), (1,)))

    arrived = [L.along_tp(rows_for((c + d) % T).astype(BF16), d) for d in range(1, T)]
    own = rows_for(c)
    for a in arrived:
        own = own + a.astype(F32)
    blocks = own.astype(BF16).reshape(C, strip, D)

    if C == 1:
        final = blocks[0].astype(F32)
    elif C == R:
        got = [pick(blocks, q)]
        for d in range(1, R):
            got.append(L.along_q(pick(blocks, (q + d) % R), d))
        rev = [got[(-k) % R] for k in range(R)]
        by_part = jnp.stack(rev)
        final = pick(by_part, (h - q) % R).astype(F32)
        for d in range(1, C):
            final = final + L.along_h(pick(by_part, (h + d - q) % R), d).astype(F32)
    else:
        final = 0.0
        for d in range(C):
            perm = [(l * R + p, p * C + (l + d) % C) for l in range(C) for p in range(R)]
            final = final + lax.ppermute(pick(blocks, (h + d) % C), "sp", perm).astype(F32)
    final = final.astype(BF16).reshape(strip, R, C, rows).transpose(0, 2, 1, 3)
    return final.reshape(strip, D)


HIGHEST = lax.Precision.HIGHEST
NT = ((1,), (1,))
TN = ((0,), (0,))


def kernel(body, outs, pos, *args, scratch=(), limit=24 << 20, alias=None, part=None, far=False):
    specs, arrays = [], []
    for a in args:
        if isinstance(a, tuple) and a[1] is None:
            a = a[0]
            specs.append(pl.BlockSpec(memory_space=pl.ANY))
        elif isinstance(a, tuple):
            a, block, index = a
            specs.append(pl.BlockSpec(block, lambda i, p, index=index: index(p)))
        else:
            specs.append(pl.BlockSpec(a.shape, lambda i, p, k=a.ndim: (0,) * k))
        arrays.append(a)
    shapes = [pltpu.HBM(s, d) if far else jax.ShapeDtypeStruct(s, d) for s, d in outs]
    if part is None:
        part = [s for s, _ in outs]
    whole = [pl.BlockSpec(s, lambda i, p, k=len(s): (0,) * k) for s in part]
    many = len(shapes) > 1
    return pl.pallas_call(
        body,
        out_shape=shapes if many else shapes[0],
        grid_spec=pltpu.PrefetchScalarGridSpec(
            num_scalar_prefetch=1,
            grid=(1,),
            in_specs=specs,
            out_specs=whole if many else whole[0],
            scratch_shapes=scratch,
        ),
        compiler_params=pltpu.CompilerParams(vmem_limit_bytes=limit),
        input_output_aliases=alias or {},
    )(pos, *arrays)


def hbm(x):
    return pltpu.with_memory_space_constraint(x, pltpu.HBM)


def three(x):
    a = x.astype(BF16).astype(F32)
    b = (x - a).astype(BF16).astype(F32)
    return a, b, x - a - b


def turned_body(pos, *refs):
    outs = refs[-4:]
    each = (len(refs) - 4) // 4
    for d, out in enumerate(outs):
        at = 0
        for w in refs[d * each : (d + 1) * each]:
            out[:, at : at + w.shape[1]] = w[...]
            at += w.shape[1]


def straight_body(pos, *refs):
    out = refs[-1]
    for l in range(out.shape[0]):
        at = 0
        for w in refs[:-1]:
            m = w.shape[1] // out.shape[0]
            out[l, :, at : at + m] = w[:, l * m : (l + 1) * m]
            at += m


def stack_body(pos, g0, g1, g2, g3, out):
    for d, g in enumerate((g0, g1, g2, g3)):
        out[lax.rem(pos[0] - d + 4, 4)] = g[...]


def norm_body(pos, tok, gain, off, share):
    C, R = 4, 4
    B, D = tok.shape
    rows = D // (C * R)
    x = tok[...].astype(F32)
    y = x * lax.rsqrt(jnp.mean(x * x, axis=1, keepdims=True) + EPS) * gain[...]
    y = y.astype(BF16)
    halves = []
    for t in range(2):
        halves.append(
            jnp.concatenate(
                [
                    y[:, (hh * R + qq) * rows : (hh * R + qq + 1) * rows]
                    for qq in (2 * t, 2 * t + 1)
                    for hh in range(C)
                ],
                axis=1,
            )
        )
    share[0:B, :] = jnp.where(pos[2] == 0, halves[0], halves[1])
    o = jnp.concatenate([off[k] for k in range(4)], axis=1)
    a, b, c = three(o)
    extra = jnp.concatenate(
        [jnp.concatenate([a, b], axis=1), jnp.concatenate([c, jnp.zeros_like(c)], axis=1)], axis=0
    )
    extra = jnp.concatenate([extra, jnp.zeros_like(extra)], axis=0)
    share[B : B + 16, :] = extra.astype(BF16)


def arrange_body(pos, g0, g1, g2, g3, own, offs):
    h = pos[0]
    B = own.shape[1]
    for d, g in enumerate((g0, g1, g2, g3)):
        j = lax.rem(h - d + 4, 4)
        own[j] = g[0:B, :]
        e = g[B : B + 16, :].astype(F32)
        row = lax.broadcasted_iota(jnp.int32, e.shape, 0)
        ab = jnp.sum(jnp.where(row == h, e, 0.0), axis=0, keepdims=True)
        cc = jnp.sum(jnp.where(row == h + 4, e, 0.0), axis=0, keepdims=True)
        n = ab.shape[1] // 2
        o = ab[:, :n] + ab[:, n:] + cc[:, :n]
        for k in range(4):
            offs[j, k : k + 1, :] = o[:, k * B : (k + 1) * B]


def fill_hidden(pos, own, other, hid):
    c = pos[2]
    n = own.shape[1] // 2
    for i in range(2):
        hid[2 * c + i] = own[:, i * n : (i + 1) * n]
        hid[2 - 2 * c + i] = other[:, i * n : (i + 1) * n]


def projected(pos, hid, pieces):
    q = pos[1]
    y = None
    for i, w in enumerate(pieces):
        t = dot(hid[q ^ i], w[...])
        y = t if y is None else y + t
    return y


def state_body(
    pos, own, other, a0, a1, a2, a3, b0, b1, b2, b3, gw, offs,
    k_out, v_out, g_out, gated, head, tail, m1, m2, m3, hid, pre_t
):
    h, q, c = pos[0], pos[1], pos[2]
    fill_hidden(pos, own, other, hid)
    R, N, _ = hid.shape
    kw = k_out.shape[1]
    n = gated.shape[1]
    y = projected(pos, hid, (a0, a1, a2, a3))
    k = (y[:, :kw].astype(BF16).astype(F32) * (kw ** (-0.5))).astype(BF16)
    k_out[...] = k
    a = y[:, kw : kw + n].astype(BF16).astype(F32)
    g = y[:, kw + n :].astype(BF16).astype(F32)
    z = (a * jax.nn.sigmoid(g)).astype(BF16)
    gated[...] = z
    head[...] = z[0:16, :]
    tail[...] = z[N - 16 :, :]
    rows = gw.shape[1] // 16
    pre = None
    for p in range(R):
        w = jnp.concatenate(
            [gw[:, (l * R + p) * rows : (l * R + p + 1) * rows] for l in range(4)], axis=1
        )
        t = dot(w, hid[p], NT)
        pre = t if pre is None else pre + t
    pre_t[...] = pre
    heads = gw.shape[0] // 4
    at = c * 4 + h
    pre = jnp.concatenate([pre_t[pl.ds(i * heads + at, 1), :] for i in range(4)], axis=0)
    off = jnp.concatenate([offs[j] for j in range(4)], axis=1)
    pre = pre + off
    lf = jnp.minimum(pre, 0.0) - jnp.log1p(jnp.exp(-jnp.abs(pre)))
    lf8 = jnp.concatenate([lf, lf], axis=0)
    ri = lax.broadcasted_iota(jnp.int32, (N, N), 0)
    ci = lax.broadcasted_iota(jnp.int32, (N, N), 1)
    up = jnp.where(ri <= ci, 1.0, 0.0).astype(BF16)
    down = jnp.where(ri >= ci, 1.0, 0.0).astype(BF16)
    f, b = None, None
    for t in three(lf8):
        t = t.astype(BF16)
        f1, b1_ = dot(t, up), dot(t, down)
        f = f1 if f is None else f + f1
        b = b1_ if b is None else b + b1_
    f, b = f[1:2], b[3:4]
    inf, inb = pre[0:1], pre[2:3]
    pf, pb = f[:, N - 1 : N], b[:, 0:1]
    tf, tb = pf - f + inf, pb - b + inb
    lvf, lvb = jnp.max(tf, axis=1, keepdims=True), jnp.max(tb, axis=1, keepdims=True)
    wf, wb = jnp.exp(tf - lvf), jnp.exp(tb - lvb)
    zero = jnp.zeros_like(f)
    g_out[...] = jnp.concatenate([f, b, inf - f, inb - b, zero, zero, zero, zero], axis=0)
    w8 = jnp.concatenate([wf, wb, zero, zero, zero, zero, zero, zero], axis=0)
    wt = w8.T
    nn = None
    for t in three(w8):
        t = dot(t.astype(BF16), k)
        nn = t if nn is None else nn + t
    v = projected(pos, hid, (b0, b1, b2, b3)).astype(BF16)
    v_out[...] = v
    v32 = v.astype(F32)
    mf = dot((v32 * wt[:, 0:1]).astype(BF16), k, TN).astype(BF16)
    mb = dot((v32 * wt[:, 1:2]).astype(BF16), k, TN).astype(BF16)

    def small(n1, lv, ps):
        wide_ = lambda x: jnp.broadcast_to(x, n1.shape)
        r = list(three(n1)) + [wide_(x) for x in three(lv)] + [wide_(x) for x in three(ps)]
        return jnp.concatenate(r + [jnp.zeros((7, n1.shape[1]), F32)], axis=0).astype(BF16)

    sf, sb = small(nn[0:1], lvf, pf), small(nn[1:2], lvb, pb)
    vw = mf.shape[0]
    for d, msg in enumerate((m1, m2, m3)):
        @pl.when(q + d + 1 < R)
        def _():
            msg[0:vw, :] = mf
            msg[vw:, :] = sf

        @pl.when(q + d + 1 >= R)
        def _():
            msg[0:vw, :] = mb
            msg[vw:, :] = sb


def conv_body(pos, gated, before, after, taps, bias, conv, stats, pad):
    N, n = gated.shape
    K = taps.shape[0]
    pad[0:16, :] = before[...].astype(F32)
    pad[16 : 16 + N, :] = gated[...].astype(F32)
    pad[16 + N : 32 + N, :] = after[...].astype(F32)
    lo = 16 - K // 2
    step = 64
    for r in range(0, N, step):
        acc = jnp.broadcast_to(bias[...], (step, n))
        for k in range(K):
            acc = acc + taps[k : k + 1, :] * pad[lo + k + r : lo + k + r + step, :]
        conv[r : r + step, :] = acc
    x = conv[...]
    ones = jnp.ones((8, n), F32)
    s1 = lax.dot_general(ones, x, (NT, ((), ())), precision=HIGHEST, preferred_element_type=F32)
    s2 = lax.dot_general(ones, x * x, (NT, ((), ())), precision=HIGHEST, preferred_element_type=F32)
    row = lax.broadcasted_iota(jnp.int32, s1.shape, 0)
    both = jnp.where(row == 0, s1, s2)
    for i in range(stats.shape[0]):
        stats[i] = both


def query_body(pos, own, other, c0, c1, c2, c3, qs, hid):
    fill_hidden(pos, own, other, hid)
    qs[...] = projected(pos, hid, (c0, c1, c2, c3)).astype(BF16)


def cell_body(
    pos, qs, k, v, g, m1, m2, m3, mem0, nrm0, lev0, gain, conv, stats, chgain, act, past
):
    h, q = pos[0], pos[1]
    N, _ = qs.shape
    vw = v.shape[1]
    got = (m1, m2, m3)
    lv, ps, nr = [], [], []
    for m in got:
        e = m[vw : vw + 16, :].astype(F32)
        nr.append(e[0:1] + e[1:2] + e[2:3])
        lv.append((e[3:4] + e[4:5] + e[5:6])[:, 0:1])
        ps.append((e[6:7] + e[7:8] + e[8:9])[:, 0:1])
    mems, nrms, runs = [], [], []
    for d in range(2):
        def ok(i):
            return q >= i + 1 if d == 0 else q < i + 1

        lvs = []
        for i in range(3):
            between = range(0, i) if d == 0 else range(i + 1, 3)
            x = lv[i]
            for m in between:
                x = x + jnp.where(ok(m), ps[m], 0.0)
            lvs.append(jnp.where(ok(i), x, LOW))
        x = lev0[d : d + 1, :]
        x = jnp.where(lax.broadcasted_iota(jnp.int32, x.shape, 1) == h, x, 0.0)
        x = jnp.sum(x, axis=1, keepdims=True)
        for m in range(3):
            x = x + jnp.where(ok(m), ps[m], 0.0)
        lvs.append(x)
        run = lvs[0]
        for y in lvs[1:]:
            run = jnp.maximum(run, y)
        ws = [jnp.exp(y - run) for y in lvs]
        mm = ws[3] * mem0[d, 0]
        nm = ws[3] * nrm0[d, pl.ds(h, 1), :]
        for i in range(3):
            mm = mm + ws[i] * got[i][0:vw, :].astype(F32)
            nm = nm + ws[i] * nr[i]
        mems.append(mm.astype(BF16))
        nrms.append(nm)
        runs.append(run)
    for d in range(2):
        past[d] = dot(qs[...], mems[d], NT)
    st = stats[0]
    for i in range(1, stats.shape[0]):
        st = st + stats[i]
    n = conv.shape[1]
    width = n * stats.shape[0]
    mean = st[0:1] / width
    var = st[1:2] / width - mean * mean
    rows = jnp.concatenate([g[0:2, :], mean, lax.rsqrt(var + EPS)], axis=0)
    turned = jnp.concatenate([rows, rows], axis=0).T
    x = (conv[...] - turned[:, 2:3]) * turned[:, 3:4] * chgain[...]
    act[:, 0:n] = (x * jax.nn.sigmoid(x)).astype(BF16)
    blk = N // 4
    for j in range(4):
        r0 = j * blk
        qb = qs[r0 : r0 + blk, :]
        q32 = qb.astype(F32)
        scores = dot(qb, k[...], NT)
        ri = lax.broadcasted_iota(jnp.int32, (blk, N), 0) + r0
        ci = lax.broadcasted_iota(jnp.int32, (blk, N), 1)
        total, both = None, None
        for d in range(2):
            fc = turned[r0 : r0 + blk, d : d + 1]
            mask = ri >= ci if d == 0 else ri <= ci
            table = jnp.where(mask, fc + g[2 + d : 3 + d, :], -jnp.inf)
            entry = fc + runs[d]
            top = jnp.maximum(jnp.max(table, axis=1, keepdims=True), entry)
            w = scores * jnp.exp(table - top)
            ew = jnp.exp(entry - top)
            den = jnp.sum(w, axis=1, keepdims=True)
            den = den + ew * jnp.sum(q32 * nrms[d], axis=1, keepdims=True)
            inv = 1.0 / jnp.maximum(jnp.abs(den), 1.0)
            w = w * inv
            total = w if total is None else total + w
            part = past[d, r0 : r0 + blk, :] * (ew * inv)
            both = part if both is None else both + part
        both = both + dot(total.astype(BF16), v[...])
        both = both * lax.rsqrt(jnp.mean(both * both, axis=1, keepdims=True) + EPS) * gain[...]
        act[r0 : r0 + blk, n:] = both.astype(BF16)


def out_body(pos, act, w0, w1, give, keep):
    c = pos[2]
    half = act.shape[1] // 2

    def rows_of(t):
        at = pl.multiple_of(t * half, half)
        return jnp.concatenate([act[p, pl.ds(at, half), :] for p in range(act.shape[0])], axis=0)

    x, y = rows_of(1 - c), rows_of(c)
    m = w0.shape[0]
    for i, w in enumerate((w0, w1)):
        give[:, i * m : (i + 1) * m] = dot(x, w[...], NT).astype(BF16)
    for i, w in enumerate((w0, w1)):
        keep[:, i * m : (i + 1) * m] = dot(y, w[...], NT)


def add_body(pos, keep, got, *outs):
    n = outs[0].shape[0]
    for d, out in enumerate(outs):
        at = pl.multiple_of(lax.rem(pos[0] + d, len(outs)) * n, n)
        out[...] = (keep[pl.ds(at, n), :] + got[pl.ds(at, n), :].astype(F32)).astype(BF16)


def last_body(pos, *refs):
    out, tiles = refs[-2:]
    q = pos[1]
    each = (len(refs) - 2) // 2
    for y in range(2):
        x = None
        for r in refs[y * each : (y + 1) * each]:
            x = r[...].astype(F32) if x is None else x + r[...].astype(F32)
        rows = x.shape[1] // 8
        for i in range(2):
            for l in range(4):
                at = i * 4 + l
                tiles[l * 4 + (q ^ (2 * y + i))] = x[:, at * rows : (at + 1) * rows]
    out[...] = jnp.concatenate([tiles[i] for i in range(16)], axis=1).astype(BF16)


def shards(
    tokens,
    norm_gain,
    conv_value_weight,
    conv_gate_weight,
    conv_kernel,
    conv_bias,
    channel_gain,
    query_weight,
    key_weight,
    value_weight,
    gate_weight,
    gate_offset,
    start_memory,
    start_norm,
    start_level,
    cell_gain,
    out_conv_weight,
    out_cell_weight,
):
    heads_here = start_level.shape[1]
    L = Layout(heads_here)
    S, T, C, R, h, q, c = L.S, L.T, L.C, L.R, L.h, L.q, L.c
    B, D = tokens.shape
    N = B * C
    rows = D // S
    kw = start_norm.shape[2]
    vw = start_memory.shape[2]
    n = conv_bias.shape[0] // C
    fits = C == R == 4 and T == 2 and heads_here == C and B % 128 == 0 and rows % 128 == 0
    fits = fits and n % 128 == 0 and kw % 128 == 0 and vw % 128 == 0 and conv_kernel.shape[0] <= 31
    if not fits:
        return shards_general(
            tokens,
            norm_gain,
            conv_value_weight,
            conv_gate_weight,
            conv_kernel,
            conv_bias,
            channel_gain,
            query_weight,
            key_weight,
            value_weight,
            gate_weight,
            gate_offset,
            start_memory,
            start_norm,
            start_level,
            cell_gain,
            out_conv_weight,
            out_cell_weight,
        )
    pos = jnp.stack([h, q, c, jnp.zeros_like(h)]).astype(jnp.int32)
    lines = [[l * R + p for l in range(C)] for p in range(R)]
    planes = [[l * R + p for p in range(R)] for l in range(C)]

    def swap(x, groups, axes="sp"):
        return lax.all_to_all(x, axes, 0, 0, axis_index_groups=groups, tiled=True)

    def flip(x, d):
        return L.flip_q(x, d)

    def at_col(x):
        m = x.shape[1] // C
        return (hbm(x), (x.shape[0], m), lambda p: (0, p[0]))

    wide = C * rows

    def turned(weights):
        blocks = [
            (hbm(w), (rows, w.shape[1] // C), lambda p, d=d: (0, lax.rem(p[0] + d, C)))
            for d in range(C)
            for w in weights
        ]
        width = sum(w.shape[1] for w in weights) // C
        return kernel(turned_body, [((rows, width), BF16)] * C, pos, *blocks)

    def straight(weights):
        width = sum(w.shape[1] for w in weights) // C
        return kernel(straight_body, [((C, rows, width), BF16)], pos, *map(hbm, weights))

    def cross(turn, place=lambda x: x):
        got = [turn[0]]
        for d in range(1, C):
            got.append(L.along_h(turn[d], d))
        shape = (C, rows, turn[0].shape[1])
        out = kernel(stack_body, [(shape, BF16)], pos, *map(place, got))
        return out.reshape(wide, -1)

    z_a = cross(turned((key_weight, conv_value_weight, conv_gate_weight)))
    z_b = swap(straight((value_weight,)), lines).reshape(wide, -1)
    share = kernel(
        norm_body,
        [((B + 16, D // 2), BF16)],
        pos,
        hbm(tokens),
        norm_gain.reshape(1, D),
        gate_offset.reshape(4, heads_here, B),
    )
    got = []
    for d in range(C):
        got.append(L.to_part(share, d))
    z_q = cross(turned((query_weight,)), hbm)
    z_o = swap(straight((out_conv_weight, out_cell_weight)), lines)
    z_o = z_o.reshape(wide, -1)

    a1, a2 = flip(z_a, 1), flip(z_a, 2)
    b1, b2 = flip(z_b, 1), flip(z_b, 2)
    a3 = flip(a1, 2)
    b3 = flip(b2, 1)
    q1, q2 = flip(z_q, 1), flip(z_q, 2)
    q3 = flip(z_q, 3)
    o1, o2 = flip(z_o, 1), flip(z_o, 2)
    o3 = flip(o1, 2)

    own, offs = kernel(arrange_body, [((C, B, D // 2), BF16), ((C, 4, B), F32)], pos, *got)
    own = own.reshape(N, D // 2)
    other = L.along_tp(own, 1)
    hid = pltpu.VMEM((R, N, wide), BF16)
    keys, values, gates, gated, head, tail, *msg = kernel(
        state_body,
        [
            ((N, kw), BF16),
            ((N, vw), BF16),
            ((8, N), F32),
            ((N, n), BF16),
            ((16, n), BF16),
            ((16, n), BF16),
        ]
        + [((vw + 16, kw), BF16)] * (R - 1),
        pos,
        own,
        other,
        z_a,
        a1,
        a2,
        a3,
        z_b,
        b1,
        b2,
        b3,
        gate_weight.T,
        offs,
        scratch=[hid, pltpu.VMEM((gate_weight.shape[1], N), F32)],
        far=True,
    )
    up = [(l * R + i, l * R + i + 1) for l in range(C) for i in range(R - 1)]
    before = lax.ppermute(tail, "sp", up)
    after = lax.ppermute(head, "sp", [(b, a) for a, b in up])
    states = []
    for d in range(1, R):
        states.append(L.along_q(msg[d - 1], d))
    conv, stats = kernel(
        conv_body,
        [((N, n), F32), ((C * T, 8, N), F32)],
        pos,
        hbm(gated),
        before,
        after,
        at_col(conv_kernel),
        at_col(conv_bias.reshape(1, C * n)),
        scratch=[pltpu.VMEM((N + 32, n), F32)],
        far=True,
    )
    stats = swap(
        stats,
        [[(l * R + p) * T + t for l in range(C) for t in range(T)] for p in range(R)],
        ("sp", "tp"),
    )
    queries = kernel(query_body, [((N, kw), BF16)], pos, own, other, z_q, q1, q2, q3, scratch=[hid])
    act = kernel(
        cell_body,
        [((N, n + vw), BF16)],
        pos,
        queries,
        hbm(keys),
        hbm(values),
        hbm(gates),
        *states,
        (hbm(start_memory), (2, 1, vw, kw), lambda p: (0, p[0], 0, 0)),
        hbm(start_norm),
        hbm(start_level),
        at_col(cell_gain.reshape(1, C * vw)),
        hbm(conv),
        stats,
        at_col(channel_gain.reshape(1, C * n)),
        scratch=[pltpu.VMEM((2, N, vw), F32)],
    )
    act = swap(act.reshape(C, B, n + vw), planes)
    ends = []
    for w0, w1 in ((z_o, o1), (o2, o3)):
        give, keep = kernel(
            out_body, [((N // 2, 2 * wide), BF16), ((N // 2, 2 * wide), F32)], pos, act, w0, w1
        )
        give = L.along_tp(give, 1)
        blocks = kernel(add_body, [((B // T, 2 * wide), BF16)] * C, pos, keep, give)
        ends.append(blocks[0])
        for d in range(1, C):
            ends.append(L.along_h(blocks[d], d))
    return kernel(
        last_body, [((B // T, D), BF16)], pos, *ends, scratch=[pltpu.VMEM((16, B // T, rows), F32)]
    )


def solution(mesh):
    in_specs = (
        P("sp", None),
        P(),
        P("sp", "tp"),
        P("sp", "tp"),
        P(None, "tp"),
        P("tp"),
        P("tp"),
        P("sp", "tp"),
        P("sp", "tp"),
        P("sp", "tp"),
        P(),
        P(None, None, "tp", "sp"),
        P(None, "tp", None, None),
        P(None, "tp", None),
        P(None, "tp"),
        P("tp"),
        P("sp", "tp"),
        P("sp", "tp"),
    )
    out_specs = P(("sp", "tp"), None)
    return jax.shard_map(shards, mesh=mesh, in_specs=in_specs, out_specs=out_specs, check_vma=False)
```

```python
import math

import jax
import jax.numpy as jnp
from jax import lax
from jax.experimental import pallas as pl
from jax.experimental.pallas import tpu as pltpu
from jax.sharding import PartitionSpec as P


EPS = 1e-06
LOW = -1e30
F32 = jnp.float32
BF16 = jnp.bfloat16


def dot(a, b, dims=((1,), (0,))):
    return lax.dot_general(a, b, (dims, ((), ())), preferred_element_type=F32)


def pick(stack, index, axis=0):
    return lax.dynamic_index_in_dim(stack, index, axis, keepdims=False)


class Layout:
    def __init__(self, heads_here):
        self.S = lax.axis_size("sp")
        self.T = lax.axis_size("tp")
        self.C = math.gcd(heads_here, self.S)
        self.R = self.S // self.C
        s = lax.axis_index("sp")
        self.h = s // self.R
        self.q = s % self.R
        self.c = lax.axis_index("tp")

    def along_h(self, x, d):
        C, R = self.C, self.R
        return lax.ppermute(
            x, "sp", [(h * R + q, (h + d) % C * R + q) for h in range(C) for q in range(R)]
        )

    def along_q(self, x, d):
        C, R = self.C, self.R
        return lax.ppermute(
            x, "sp", [(h * R + q, h * R + (q + d) % R) for h in range(C) for q in range(R)]
        )

    def flip_q(self, x, d):
        C, R = self.C, self.R
        return lax.ppermute(
            x, "sp", [(h * R + q, h * R + (q ^ d)) for h in range(C) for q in range(R)]
        )

    def along_tp(self, x, d):
        T = self.T
        return lax.ppermute(x, "tp", [(c, (c + d) % T) for c in range(T)])

    def to_part(self, x, d):
        C, R = self.C, self.R
        return lax.ppermute(
            x, "sp", [(s, (s % C + d) % C * R + s // C) for s in range(self.S)]
        )

    def spread_heads(self, chunks_of):
        C = self.C
        got = [chunks_of(self.h)]
        for d in range(1, C):
            got.append(self.along_h(chunks_of((self.h + d) % C), d))
        rev = [got[(-k) % C] for k in range(C)]
        if C == 1:
            return rev[0][None]
        twice = jnp.stack(rev + rev)
        return lax.dynamic_slice_in_dim(twice, (C - self.h) % C, C, 0)

    def gather_parts(self, x):
        R = self.R
        n = x.shape[0]
        if R == 4 and n % 2 == 0:
            a = self.flip_q(x, 1)
            b = self.flip_q(x, 2)
            m = n // 2
            c = self.flip_q(a[:m], 2)
            d = self.flip_q(b[m:], 1)
            return [
                (self.q, 0, n, x),
                (self.q ^ 1, 0, n, a),
                (self.q ^ 2, 0, n, b),
                (self.q ^ 3, 0, m, c),
                (self.q ^ 3, m, n, d),
            ]
        if R <= 8:
            return [(self.q, 0, n, x)] + [
                ((self.q - d) % R, 0, n, self.along_q(x, d)) for d in range(1, R)
            ]
        groups = [[h * R + q for q in range(R)] for h in range(self.C)]
        g = lax.all_gather(x, "sp", axis=0, axis_index_groups=groups, tiled=False)
        return [(q, 0, n, g[q]) for q in range(R)]


def shards_general(
    tokens,
    norm_gain,
    conv_value_weight,
    conv_gate_weight,
    conv_kernel,
    conv_bias,
    channel_gain,
    query_weight,
    key_weight,
    value_weight,
    gate_weight,
    gate_offset,
    start_memory,
    start_norm,
    start_level,
    cell_gain,
    out_conv_weight,
    out_cell_weight,
):
    heads_here = start_level.shape[1]
    L = Layout(heads_here)
    S, T, C, R, h, q, c = L.S, L.T, L.C, L.R, L.h, L.q, L.c
    HL = heads_here // C
    B = tokens.shape[0]
    D = tokens.shape[1]
    N = B * C
    rows = D // S
    key_width = start_norm.shape[2]
    value_width = start_memory.shape[2]
    chan = conv_bias.shape[0] // C
    conv_all = conv_bias.shape[0] * T

    def mine(x, axis):
        n = x.shape[axis] // C
        return lax.dynamic_slice_in_dim(x, h * n, n, axis)

    features = tokens.astype(F32)
    normed = (
        features * lax.rsqrt(jnp.mean(features * features, axis=1, keepdims=True) + EPS) * norm_gain
    ).astype(BF16)
    normed = normed.reshape(B, C, R, rows).transpose(0, 2, 1, 3).reshape(B, D)
    half = D // T
    share = lax.dynamic_slice_in_dim(normed, c * half, half, 1)

    def columns(weights, line):
        return jnp.concatenate(
            [
                lax.dynamic_slice_in_dim(w, line * (w.shape[1] // C), w.shape[1] // C, 1)
                for w in weights
            ],
            axis=1,
        )

    def first(weights):
        got = L.spread_heads(lambda line: columns(weights, line))
        return got.reshape(C * rows, got.shape[2])

    conv_piece = first((conv_value_weight, conv_gate_weight))
    key_piece = first((key_weight,))
    value_piece = first((value_weight,))
    query_piece = first((query_weight,))

    got_tokens = [L.to_part(share, d) if C > 1 else share for d in range(C)]
    offsets = gate_offset.reshape(2, 2, C, HL, B)
    j_here = lax.axis_index("sp") % C
    got_offset = [
        L.to_part(pick(offsets, (j_here + d) % C, 2), d) if C > 1 else offsets[:, :, 0]
        for d in range(C)
    ]

    def in_order(got, axis):
        if C == 1:
            return got[0]
        rev = [got[(-k) % C] for k in range(C)]
        twice = jnp.concatenate(rev + rev, axis=axis)
        n = got[0].shape[axis]
        return lax.dynamic_slice_in_dim(twice, (C - h) % C * n, C * n, axis)

    share_all = in_order(got_tokens, 0)
    offset_all = in_order(got_offset, 3)
    others = [L.along_tp(share_all, d) for d in range(1, T)]
    parts = [share_all] + others
    rev = [parts[(-k) % T] for k in range(T)]
    hidden = lax.dynamic_slice_in_dim(
        jnp.concatenate(rev + rev, axis=1), (T - c) % T * half, D, 1
    )

    wide = C * rows

    def project(piece):
        total = None
        for part, lo, hi, w in L.gather_parts(piece):
            x = lax.dynamic_slice_in_dim(hidden, part * wide + lo, hi - lo, 1)
            y = dot(x, w)
            total = y if total is None else total + y
        return total

    conv_pre = project(conv_piece).astype(BF16)
    keys = project(key_piece).astype(BF16)
    values = project(value_piece).astype(BF16)
    queries = project(query_piece).astype(BF16)

    out_piece = L.spread_heads(
        lambda line: columns((out_conv_weight, out_cell_weight), line)
    ).reshape(C * rows, -1)
    out_rows = jnp.zeros((D, out_piece.shape[1]), BF16)
    for part, lo, hi, w in L.gather_parts(out_piece):
        out_rows = lax.dynamic_update_slice(out_rows, w, (part * wide + lo, 0))

    conv_value = conv_pre[:, :chan].astype(F32)
    conv_gate = conv_pre[:, chan:].astype(F32)
    gated = (conv_value * jax.nn.sigmoid(conv_gate)).astype(BF16)
    reach = conv_kernel.shape[0] // 2
    line_up = [(l * R + i, l * R + i + 1) for l in range(C) for i in range(R - 1)]
    before = lax.ppermute(gated[N - reach :], "sp", line_up)
    after = lax.ppermute(gated[:reach], "sp", [(b, a) for a, b in line_up])
    padded = jnp.concatenate([before, gated, after], axis=0).astype(F32)
    taps = mine(conv_kernel, 1)
    conv_sum = mine(conv_bias, 0) + sum(
        taps[k] * padded[k : k + N] for k in range(taps.shape[0])
    )
    stats = jnp.stack([jnp.sum(conv_sum, axis=1), jnp.sum(conv_sum * conv_sum, axis=1)])
    total = stats
    for d in range(C):
        for e in range(T):
            if d or e:
                total = total + lax.ppermute(
                    stats,
                    ("sp", "tp"),
                    [
                        ((l * R + p) * T + t, ((l + d) % C * R + p) * T + (t + e) % T)
                        for l in range(C)
                        for p in range(R)
                        for t in range(T)
                    ],
                )
    mean = total[0] / conv_all
    var = total[1] / conv_all - mean * mean
    conv_out = jax.nn.silu(
        (conv_sum - mean[:, None]) * lax.rsqrt(var + EPS)[:, None] * mine(channel_gain, 0)
    ).astype(BF16)

    groups = gate_weight.shape[1] // 4
    gates_w = gate_weight.reshape(C, R, rows, 4, groups)
    gates_w = lax.dynamic_slice_in_dim(gates_w, c * heads_here + h * HL, HL, 4)
    gates_w = gates_w.transpose(1, 0, 2, 3, 4).reshape(D, 4 * HL)
    gate_pre = dot(gates_w, hidden, ((0,), (1,))).reshape(2, 2, HL, N) + offset_all
    in_gate = gate_pre[:, 0]
    log_forget = jax.nn.log_sigmoid(gate_pre[:, 1])
    upto = (jnp.arange(N)[:, None] <= jnp.arange(N)[None, :]).astype(F32)
    forward_sum = jnp.dot(log_forget[0], upto, precision=lax.Precision.HIGHEST)
    backward_sum = jnp.dot(log_forget[1], upto.T, precision=lax.Precision.HIGHEST)
    sums = jnp.stack([forward_sum, backward_sum])
    passed = jnp.stack([forward_sum[:, -1], backward_sum[:, 0]])
    tail = passed[:, :, None] - sums + in_gate
    level = jnp.max(tail, axis=2)
    new_weight = jnp.exp(tail - level[:, :, None])
    my_memory = mine(start_memory, 1)
    my_norm = mine(start_norm, 1)
    my_level = mine(start_level, 1)
    step = jnp.arange(N)
    cells = []
    scale = key_width ** (-0.5)
    for i in range(HL):
        k = keys[:, i * key_width : (i + 1) * key_width] * jnp.asarray(scale, BF16)
        v = values[:, i * value_width : (i + 1) * value_width]
        qr = queries[:, i * key_width : (i + 1) * key_width]
        memories = []
        norms = []
        for d in range(2):
            w = new_weight[d, i]
            memories.append(dot((v.astype(F32) * w[:, None]).astype(BF16), k, ((0,), (0,))))
            norms.append(jnp.sum(w[:, None] * k.astype(F32), axis=0))
        memories = jnp.stack(memories).astype(BF16)
        smalls = jnp.concatenate(
            [jnp.stack(norms), level[:, i, None], passed[:, i, None]], axis=1
        )
        if R <= 8:
            got = []
            for d in range(1, R):
                back = jnp.where(q + d < R, 0, 1)
                got.append(
                    (L.along_q(pick(memories, back), d), L.along_q(pick(smalls, back), d))
                )
            get = lambda direction, dist: got[dist - 1 if direction == 0 else R - dist - 1]
        else:
            groups_q = [[l * R + p for p in range(R)] for l in range(C)]
            all_m = lax.all_gather(memories, "sp", axis=0, axis_index_groups=groups_q)
            all_s = lax.all_gather(smalls, "sp", axis=0, axis_index_groups=groups_q)

            def get(direction, dist):
                p = (q - dist) % R if direction == 0 else (q + dist) % R
                return pick(all_m, p)[direction], pick(all_s, p)[direction]

        scores = dot(qr, k, ((1,), (1,)))
        table_sum = None
        carried = None
        for direction in range(2):
            levels, mems, nrms = [], [], []
            decay = jnp.zeros((), F32)
            for dist in range(1, R):
                m, sm = get(direction, dist)
                there = q >= dist if direction == 0 else q + dist < R
                levels.append(jnp.where(there, sm[-2] + decay, LOW))
                mems.append(m)
                nrms.append(sm[:-2])
                decay = decay + jnp.where(there, sm[-1], 0.0)
            levels.append(my_level[direction, i] + decay)
            mems.append(my_memory[direction, i])
            nrms.append(my_norm[direction, i])
            run_level = levels[0]
            for lv in levels[1:]:
                run_level = jnp.maximum(run_level, lv)
            ws = [jnp.exp(lv - run_level) for lv in levels]
            memory = sum(w * m.astype(F32) for w, m in zip(ws, mems)).astype(BF16)
            norm = sum(w * n for w, n in zip(ws, nrms))
            f = sums[direction, i]
            g = in_gate[direction, i]
            mask = step[:, None] >= step[None, :] if direction == 0 else step[:, None] <= step[None, :]
            table = jnp.where(mask, f[:, None] + (g - f)[None, :], -jnp.inf)
            entry = f + run_level
            top = jnp.maximum(jnp.max(table, axis=1), entry)
            weights = scores * jnp.exp(table - top[:, None])
            ew = jnp.exp(entry - top)
            qn = jnp.sum(qr.astype(F32) * norm[None, :], axis=1)
            den = jnp.sum(weights, axis=1) + ew * qn
            inv = 1.0 / jnp.maximum(jnp.abs(den), 1.0)
            scaled = weights * inv[:, None]
            table_sum = scaled if table_sum is None else table_sum + scaled
            part = dot(qr, memory, ((1,), (1,))) * (ew * inv)[:, None]
            carried = part if carried is None else carried + part
        both = dot(table_sum.astype(BF16), v) + carried
        both = both * lax.rsqrt(jnp.mean(both * both, axis=1, keepdims=True) + EPS)
        gain = lax.dynamic_slice_in_dim(mine(cell_gain, 0), i * value_width, value_width, 0)
        cells.append((both * gain).astype(BF16))

    act = jnp.concatenate([conv_out] + cells, axis=1)
    strip = B // T
    act = act.reshape(C, T, strip, act.shape[1])

    def rows_for(t):
        x = pick(act, t, 1).reshape(C * strip, act.shape[3])
        return dot(x, out_rows, ((1,), (1,)))

    arrived = [L.along_tp(rows_for((c + d) % T).astype(BF16), d) for d in range(1, T)]
    own = rows_for(c)
    for a in arrived:
        own = own + a.astype(F32)
    blocks = own.astype(BF16).reshape(C, strip, D)

    if C == 1:
        final = blocks[0].astype(F32)
    elif C == R:
        got = [pick(blocks, q)]
        for d in range(1, R):
            got.append(L.along_q(pick(blocks, (q + d) % R), d))
        rev = [got[(-k) % R] for k in range(R)]
        by_part = jnp.stack(rev)
        final = pick(by_part, (h - q) % R).astype(F32)
        for d in range(1, C):
            final = final + L.along_h(pick(by_part, (h + d - q) % R), d).astype(F32)
    else:
        final = 0.0
        for d in range(C):
            perm = [(l * R + p, p * C + (l + d) % C) for l in range(C) for p in range(R)]
            final = final + lax.ppermute(pick(blocks, (h + d) % C), "sp", perm).astype(F32)
    final = final.astype(BF16).reshape(strip, R, C, rows).transpose(0, 2, 1, 3)
    return final.reshape(strip, D)


HIGHEST = lax.Precision.HIGHEST
NT = ((1,), (1,))


def kernel(body, outs, pos, *args, scratch=(), limit=24 << 20, alias=None, part=None, far=False):
    specs, arrays = [], []
    for a in args:
        if isinstance(a, tuple) and a[1] is None:
            a = a[0]
            specs.append(pl.BlockSpec(memory_space=pl.ANY))
        elif isinstance(a, tuple):
            a, block, index = a
            specs.append(pl.BlockSpec(block, lambda i, p, index=index: index(p)))
        else:
            specs.append(pl.BlockSpec(a.shape, lambda i, p, k=a.ndim: (0,) * k))
        arrays.append(a)
    shapes = [pltpu.HBM(s, d) if far else jax.ShapeDtypeStruct(s, d) for s, d in outs]
    if part is None:
        part = [s for s, _ in outs]
    whole = [pl.BlockSpec(s, lambda i, p, k=len(s): (0,) * k) for s in part]
    many = len(shapes) > 1
    return pl.pallas_call(
        body,
        out_shape=shapes if many else shapes[0],
        grid_spec=pltpu.PrefetchScalarGridSpec(
            num_scalar_prefetch=1,
            grid=(1,),
            in_specs=specs,
            out_specs=whole if many else whole[0],
            scratch_shapes=scratch,
        ),
        compiler_params=pltpu.CompilerParams(vmem_limit_bytes=limit),
        input_output_aliases=alias or {},
    )(pos, *arrays)


def hbm(x):
    return pltpu.with_memory_space_constraint(x, pltpu.HBM)


def three(x):
    a = x.astype(BF16).astype(F32)
    b = (x - a).astype(BF16).astype(F32)
    return a, b, x - a - b


def turned_body(pos, *refs):
    outs = refs[-4:]
    each = (len(refs) - 4) // 4
    for d, out in enumerate(outs):
        at = 0
        for w in refs[d * each : (d + 1) * each]:
            out[:, at : at + w.shape[1]] = w[...]
            at += w.shape[1]


def straight_body(pos, *refs):
    out = refs[-1]
    for l in range(out.shape[0]):
        at = 0
        for w in refs[:-1]:
            m = w.shape[1] // out.shape[0]
            out[l, :, at : at + m] = w[:, l * m : (l + 1) * m]
            at += m


def stack_body(pos, g0, g1, g2, g3, out):
    for d, g in enumerate((g0, g1, g2, g3)):
        out[lax.rem(pos[0] - d + 4, 4)] = g[...]


def norm_body(pos, tok, gain, off, share):
    C, R = 4, 4
    B, D = tok.shape
    rows = D // (C * R)
    x = tok[...].astype(F32)
    y = x * lax.rsqrt(jnp.mean(x * x, axis=1, keepdims=True) + EPS) * gain[...]
    y = y.astype(BF16)
    halves = []
    for t in range(2):
        halves.append(
            jnp.concatenate(
                [
                    y[:, (hh * R + qq) * rows : (hh * R + qq + 1) * rows]
                    for qq in (2 * t, 2 * t + 1)
                    for hh in range(C)
                ],
                axis=1,
            )
        )
    share[0:B, :] = jnp.where(pos[2] == 0, halves[0], halves[1])
    o = jnp.concatenate([off[k] for k in range(4)], axis=1)
    a, b, c = three(o)
    extra = jnp.concatenate(
        [jnp.concatenate([a, b], axis=1), jnp.concatenate([c, jnp.zeros_like(c)], axis=1)], axis=0
    )
    extra = jnp.concatenate([extra, jnp.zeros_like(extra)], axis=0)
    share[B : B + 16, :] = extra.astype(BF16)


def arrange_body(pos, g0, g1, g2, g3, own, offs):
    h = pos[0]
    B = own.shape[1]
    for d, g in enumerate((g0, g1, g2, g3)):
        j = lax.rem(h - d + 4, 4)
        own[j] = g[0:B, :]
        e = g[B : B + 16, :].astype(F32)
        row = lax.broadcasted_iota(jnp.int32, e.shape, 0)
        ab = jnp.sum(jnp.where(row == h, e, 0.0), axis=0, keepdims=True)
        cc = jnp.sum(jnp.where(row == h + 4, e, 0.0), axis=0, keepdims=True)
        n = ab.shape[1] // 2
        o = ab[:, :n] + ab[:, n:] + cc[:, :n]
        for k in range(4):
            offs[j, k : k + 1, :] = o[:, k * B : (k + 1) * B]


def fill_hidden(pos, own, other, hid):
    c = pos[2]
    n = own.shape[1] // 2
    for i in range(2):
        hid[2 * c + i] = own[:, i * n : (i + 1) * n]
        hid[2 - 2 * c + i] = other[:, i * n : (i + 1) * n]


def projected(pos, hid, pieces):
    q = pos[1]
    y = None
    for i, w in enumerate(pieces):
        t = dot(hid[q ^ i], w[...])
        y = t if y is None else y + t
    return y


def state_body(
    pos, own, other, a0, a1, a2, a3, b0, b1, b2, b3, gw, offs,
    k_out, v_out, g_out, gated, head, tail, m1, m2, m3, hid, pre_t
):
    h, q, c = pos[0], pos[1], pos[2]
    fill_hidden(pos, own, other, hid)
    R, N, _ = hid.shape
    kw = k_out.shape[1]
    n = gated.shape[1]
    y = projected(pos, hid, (a0, a1, a2, a3))
    k = (y[:, :kw].astype(BF16).astype(F32) * (kw ** (-0.5))).astype(BF16)
    k_out[...] = k
    a = y[:, kw : kw + n].astype(BF16).astype(F32)
    g = y[:, kw + n :].astype(BF16).astype(F32)
    z = (a * jax.nn.sigmoid(g)).astype(BF16)
    gated[...] = z
    head[...] = z[0:16, :]
    tail[...] = z[N - 16 :, :]
    rows = gw.shape[1] // 16
    pre = None
    for p in range(R):
        w = jnp.concatenate(
            [gw[:, (l * R + p) * rows : (l * R + p + 1) * rows] for l in range(4)], axis=1
        )
        t = dot(w, hid[p], NT)
        pre = t if pre is None else pre + t
    pre_t[...] = pre
    heads = gw.shape[0] // 4
    at = c * 4 + h
    pre = jnp.concatenate([pre_t[pl.ds(i * heads + at, 1), :] for i in range(4)], axis=0)
    off = jnp.concatenate([offs[j] for j in range(4)], axis=1)
    pre = pre + off
    lf = jnp.minimum(pre, 0.0) - jnp.log1p(jnp.exp(-jnp.abs(pre)))
    lf8 = jnp.concatenate([lf, lf], axis=0)
    ri = lax.broadcasted_iota(jnp.int32, (N, N), 0)
    ci = lax.broadcasted_iota(jnp.int32, (N, N), 1)
    up = jnp.where(ri <= ci, 1.0, 0.0).astype(BF16)
    down = jnp.where(ri >= ci, 1.0, 0.0).astype(BF16)
    f, b = None, None
    for t in three(lf8):
        t = t.astype(BF16)
        f1, b1_ = dot(t, up), dot(t, down)
        f = f1 if f is None else f + f1
        b = b1_ if b is None else b + b1_
    f, b = f[1:2], b[3:4]
    inf, inb = pre[0:1], pre[2:3]
    pf, pb = f[:, N - 1 : N], b[:, 0:1]
    tf, tb = pf - f + inf, pb - b + inb
    lvf, lvb = jnp.max(tf, axis=1, keepdims=True), jnp.max(tb, axis=1, keepdims=True)
    wf, wb = jnp.exp(tf - lvf), jnp.exp(tb - lvb)
    zero = jnp.zeros_like(f)
    g_out[...] = jnp.concatenate([f, b, inf - f, inb - b, zero, zero, zero, zero], axis=0)
    w8 = jnp.concatenate([wf, wb, zero, zero, zero, zero, zero, zero], axis=0)
    nn = None
    for t in three(w8):
        t = dot(t.astype(BF16), k)
        nn = t if nn is None else nn + t
    v = projected(pos, hid, (b0, b1, b2, b3)).astype(BF16)
    v_out[...] = v
    kt = k.astype(F32).T
    mf = dot((kt * wf).astype(BF16), v).astype(BF16)
    mb = dot((kt * wb).astype(BF16), v).astype(BF16)

    def small(n1, lv, ps):
        n1 = jnp.concatenate([n1, jnp.zeros((1, v.shape[1] - n1.shape[1]), F32)], axis=1)
        wide_ = lambda x: jnp.broadcast_to(x, n1.shape)
        r = list(three(n1)) + [wide_(x) for x in three(lv)] + [wide_(x) for x in three(ps)]
        return jnp.concatenate(r + [jnp.zeros((7, n1.shape[1]), F32)], axis=0).astype(BF16)

    sf, sb = small(nn[0:1], lvf, pf), small(nn[1:2], lvb, pb)
    for d, msg in enumerate((m1, m2, m3)):
        @pl.when(q + d + 1 < R)
        def _():
            msg[0:kw, :] = mf
            msg[kw:, :] = sf

        @pl.when(q + d + 1 >= R)
        def _():
            msg[0:kw, :] = mb
            msg[kw:, :] = sb


def conv_body(pos, gated, before, after, taps, bias, conv, stats, pad):
    N, n = gated.shape
    K = taps.shape[0]
    pad[0:16, :] = before[...].astype(F32)
    pad[16 : 16 + N, :] = gated[...].astype(F32)
    pad[16 + N : 32 + N, :] = after[...].astype(F32)
    lo = 16 - K // 2
    step = 64
    for r in range(0, N, step):
        acc = jnp.broadcast_to(bias[...], (step, n))
        for k in range(K):
            acc = acc + taps[k : k + 1, :] * pad[lo + k + r : lo + k + r + step, :]
        conv[r : r + step, :] = acc
    x = conv[...]
    ones = jnp.ones((8, n), F32)
    s1 = lax.dot_general(ones, x, (NT, ((), ())), precision=HIGHEST, preferred_element_type=F32)
    s2 = lax.dot_general(ones, x * x, (NT, ((), ())), precision=HIGHEST, preferred_element_type=F32)
    row = lax.broadcasted_iota(jnp.int32, s1.shape, 0)
    both = jnp.where(row == 0, s1, s2)
    for i in range(stats.shape[0]):
        stats[i] = both


def query_body(pos, own, other, c0, c1, c2, c3, qs, hid):
    fill_hidden(pos, own, other, hid)
    qs[...] = projected(pos, hid, (c0, c1, c2, c3)).astype(BF16)


def cell_body(
    pos, qs, k, v, g, m1, m2, m3, mem0, nrm0, lev0, gain, conv, stats, chgain, act, past
):
    h, q = pos[0], pos[1]
    N, kw = qs.shape
    got = (m1, m2, m3)
    lv, ps, nr = [], [], []
    for m in got:
        e = m[kw : kw + 16, :].astype(F32)
        nr.append((e[0:1] + e[1:2] + e[2:3])[:, 0:kw])
        lv.append((e[3:4] + e[4:5] + e[5:6])[:, 0:1])
        ps.append((e[6:7] + e[7:8] + e[8:9])[:, 0:1])
    nrms, runs = [], []
    for d in range(2):
        def ok(i):
            return q >= i + 1 if d == 0 else q < i + 1

        lvs = []
        for i in range(3):
            between = range(0, i) if d == 0 else range(i + 1, 3)
            x = lv[i]
            for m in between:
                x = x + jnp.where(ok(m), ps[m], 0.0)
            lvs.append(jnp.where(ok(i), x, LOW))
        x = lev0[d : d + 1, :]
        x = jnp.where(lax.broadcasted_iota(jnp.int32, x.shape, 1) == h, x, 0.0)
        x = jnp.sum(x, axis=1, keepdims=True)
        for m in range(3):
            x = x + jnp.where(ok(m), ps[m], 0.0)
        lvs.append(x)
        run = lvs[0]
        for y in lvs[1:]:
            run = jnp.maximum(run, y)
        ws = [jnp.exp(y - run) for y in lvs]
        mm = None
        nm = ws[3] * nrm0[d, pl.ds(h, 1), :]
        for i in range(3):
            t = ws[i] * got[i][0:kw, :].astype(F32)
            mm = t if mm is None else mm + t
            nm = nm + ws[i] * nr[i]
        past[d] = dot(qs[...], mm.astype(BF16)) + dot(
            qs[...], (ws[3] * mem0[d, 0]).astype(BF16), NT
        )
        nrms.append(nm)
        runs.append(run)
    st = stats[0]
    for i in range(1, stats.shape[0]):
        st = st + stats[i]
    n = conv.shape[1]
    width = n * stats.shape[0]
    mean = st[0:1] / width
    var = st[1:2] / width - mean * mean
    rows = jnp.concatenate([g[0:2, :], mean, lax.rsqrt(var + EPS)], axis=0)
    turned = jnp.concatenate([rows, rows], axis=0).T
    x = (conv[...] - turned[:, 2:3]) * turned[:, 3:4] * chgain[...]
    act[:, 0:n] = (x * jax.nn.sigmoid(x)).astype(BF16)
    blk = N // 4
    for j in range(4):
        r0 = j * blk
        qb = qs[r0 : r0 + blk, :]
        q32 = qb.astype(F32)
        scores = dot(qb, k[...], NT)
        ri = lax.broadcasted_iota(jnp.int32, (blk, N), 0) + r0
        ci = lax.broadcasted_iota(jnp.int32, (blk, N), 1)
        total, both = None, None
        for d in range(2):
            fc = turned[r0 : r0 + blk, d : d + 1]
            mask = ri >= ci if d == 0 else ri <= ci
            table = jnp.where(mask, fc + g[2 + d : 3 + d, :], -jnp.inf)
            entry = fc + runs[d]
            top = jnp.maximum(jnp.max(table, axis=1, keepdims=True), entry)
            w = scores * jnp.exp(table - top)
            ew = jnp.exp(entry - top)
            den = jnp.sum(w, axis=1, keepdims=True)
            den = den + ew * jnp.sum(q32 * nrms[d], axis=1, keepdims=True)
            inv = 1.0 / jnp.maximum(jnp.abs(den), 1.0)
            w = w * inv
            total = w if total is None else total + w
            part = past[d, r0 : r0 + blk, :] * (ew * inv)
            both = part if both is None else both + part
        both = both + dot(total.astype(BF16), v[...])
        both = both * lax.rsqrt(jnp.mean(both * both, axis=1, keepdims=True) + EPS) * gain[...]
        act[r0 : r0 + blk, n:] = both.astype(BF16)


def out_body(pos, act, w0, w1, give, keep):
    c = pos[2]
    half = act.shape[1] // 2

    def rows_of(t):
        at = pl.multiple_of(t * half, half)
        return jnp.concatenate([act[p, pl.ds(at, half), :] for p in range(act.shape[0])], axis=0)

    x, y = rows_of(1 - c), rows_of(c)
    m = w0.shape[0]
    for i, w in enumerate((w0, w1)):
        give[:, i * m : (i + 1) * m] = dot(x, w[...], NT).astype(BF16)
    for i, w in enumerate((w0, w1)):
        keep[:, i * m : (i + 1) * m] = dot(y, w[...], NT)


def add_body(pos, keep, got, *outs):
    n = outs[0].shape[0]
    for d, out in enumerate(outs):
        at = pl.multiple_of(lax.rem(pos[0] + d, len(outs)) * n, n)
        out[...] = (keep[pl.ds(at, n), :] + got[pl.ds(at, n), :].astype(F32)).astype(BF16)


def last_body(pos, *refs):
    out, tiles = refs[-2:]
    q = pos[1]
    each = (len(refs) - 2) // 2
    for y in range(2):
        x = None
        for r in refs[y * each : (y + 1) * each]:
            x = r[...].astype(F32) if x is None else x + r[...].astype(F32)
        rows = x.shape[1] // 8
        for i in range(2):
            for l in range(4):
                at = i * 4 + l
                tiles[l * 4 + (q ^ (2 * y + i))] = x[:, at * rows : (at + 1) * rows]
    out[...] = jnp.concatenate([tiles[i] for i in range(16)], axis=1).astype(BF16)


def shards(
    tokens,
    norm_gain,
    conv_value_weight,
    conv_gate_weight,
    conv_kernel,
    conv_bias,
    channel_gain,
    query_weight,
    key_weight,
    value_weight,
    gate_weight,
    gate_offset,
    start_memory,
    start_norm,
    start_level,
    cell_gain,
    out_conv_weight,
    out_cell_weight,
):
    heads_here = start_level.shape[1]
    L = Layout(heads_here)
    S, T, C, R, h, q, c = L.S, L.T, L.C, L.R, L.h, L.q, L.c
    B, D = tokens.shape
    N = B * C
    rows = D // S
    kw = start_norm.shape[2]
    vw = start_memory.shape[2]
    n = conv_bias.shape[0] // C
    fits = C == R == 4 and T == 2 and heads_here == C and B % 128 == 0 and rows % 128 == 0
    fits = fits and kw <= vw and n % 128 == 0 and kw % 128 == 0 and vw % 128 == 0 and conv_kernel.shape[0] <= 31
    if not fits:
        return shards_general(
            tokens,
            norm_gain,
            conv_value_weight,
            conv_gate_weight,
            conv_kernel,
            conv_bias,
            channel_gain,
            query_weight,
            key_weight,
            value_weight,
            gate_weight,
            gate_offset,
            start_memory,
            start_norm,
            start_level,
            cell_gain,
            out_conv_weight,
            out_cell_weight,
        )
    pos = jnp.stack([h, q, c, jnp.zeros_like(h)]).astype(jnp.int32)
    lines = [[l * R + p for l in range(C)] for p in range(R)]
    planes = [[l * R + p for p in range(R)] for l in range(C)]

    def swap(x, groups, axes="sp"):
        return lax.all_to_all(x, axes, 0, 0, axis_index_groups=groups, tiled=True)

    def flip(x, d):
        return L.flip_q(x, d)

    def at_col(x):
        m = x.shape[1] // C
        return (hbm(x), (x.shape[0], m), lambda p: (0, p[0]))

    wide = C * rows

    def turned(weights):
        blocks = [
            (hbm(w), (rows, w.shape[1] // C), lambda p, d=d: (0, lax.rem(p[0] + d, C)))
            for d in range(C)
            for w in weights
        ]
        width = sum(w.shape[1] for w in weights) // C
        return kernel(turned_body, [((rows, width), BF16)] * C, pos, *blocks)

    def straight(weights):
        width = sum(w.shape[1] for w in weights) // C
        return kernel(straight_body, [((C, rows, width), BF16)], pos, *map(hbm, weights))

    def cross(turn, place=lambda x: x):
        got = [turn[0]]
        for d in range(1, C):
            got.append(L.along_h(turn[d], d))
        shape = (C, rows, turn[0].shape[1])
        out = kernel(stack_body, [(shape, BF16)], pos, *map(place, got))
        return out.reshape(wide, -1)

    z_a = cross(turned((key_weight, conv_value_weight, conv_gate_weight)))
    z_b = swap(straight((value_weight,)), lines).reshape(wide, -1)
    share = kernel(
        norm_body,
        [((B + 16, D // 2), BF16)],
        pos,
        hbm(tokens),
        norm_gain.reshape(1, D),
        gate_offset.reshape(4, heads_here, B),
    )
    got = []
    for d in range(C):
        got.append(L.to_part(share, d))
    z_q = cross(turned((query_weight,)), hbm)
    z_o = swap(straight((out_conv_weight, out_cell_weight)), lines)
    z_o = z_o.reshape(wide, -1)

    a1, a2 = flip(z_a, 1), flip(z_a, 2)
    b1, b2 = flip(z_b, 1), flip(z_b, 2)
    a3 = flip(a1, 2)
    b3 = flip(b2, 1)
    q1, q2 = flip(z_q, 1), flip(z_q, 2)
    q3 = flip(z_q, 3)
    o1, o2 = flip(z_o, 1), flip(z_o, 2)
    o3 = flip(o1, 2)

    own, offs = kernel(arrange_body, [((C, B, D // 2), BF16), ((C, 4, B), F32)], pos, *got)
    own = own.reshape(N, D // 2)
    other = L.along_tp(own, 1)
    hid = pltpu.VMEM((R, N, wide), BF16)
    keys, values, gates, gated, head, tail, *msg = kernel(
        state_body,
        [
            ((N, kw), BF16),
            ((N, vw), BF16),
            ((8, N), F32),
            ((N, n), BF16),
            ((16, n), BF16),
            ((16, n), BF16),
        ]
        + [((kw + 16, vw), BF16)] * (R - 1),
        pos,
        own,
        other,
        z_a,
        a1,
        a2,
        a3,
        z_b,
        b1,
        b2,
        b3,
        gate_weight.T,
        offs,
        scratch=[hid, pltpu.VMEM((gate_weight.shape[1], N), F32)],
        far=True,
    )
    up = [(l * R + i, l * R + i + 1) for l in range(C) for i in range(R - 1)]
    before = lax.ppermute(tail, "sp", up)
    after = lax.ppermute(head, "sp", [(b, a) for a, b in up])
    states = []
    for d in range(1, R):
        states.append(L.along_q(msg[d - 1], d))
    conv, stats = kernel(
        conv_body,
        [((N, n), F32), ((C * T, 8, N), F32)],
        pos,
        hbm(gated),
        before,
        after,
        at_col(conv_kernel),
        at_col(conv_bias.reshape(1, C * n)),
        scratch=[pltpu.VMEM((N + 32, n), F32)],
        far=True,
    )
    stats = swap(
        stats,
        [[(l * R + p) * T + t for l in range(C) for t in range(T)] for p in range(R)],
        ("sp", "tp"),
    )
    queries = kernel(query_body, [((N, kw), BF16)], pos, own, other, z_q, q1, q2, q3, scratch=[hid])
    act = kernel(
        cell_body,
        [((N, n + vw), BF16)],
        pos,
        queries,
        hbm(keys),
        hbm(values),
        hbm(gates),
        *states,
        (hbm(start_memory), (2, 1, vw, kw), lambda p: (0, p[0], 0, 0)),
        hbm(start_norm),
        hbm(start_level),
        at_col(cell_gain.reshape(1, C * vw)),
        hbm(conv),
        stats,
        at_col(channel_gain.reshape(1, C * n)),
        scratch=[pltpu.VMEM((2, N, vw), F32)],
    )
    act = swap(act.reshape(C, B, n + vw), planes)
    ends = []
    for w0, w1 in ((z_o, o1), (o2, o3)):
        give, keep = kernel(
            out_body, [((N // 2, 2 * wide), BF16), ((N // 2, 2 * wide), F32)], pos, act, w0, w1
        )
        give = L.along_tp(give, 1)
        blocks = kernel(add_body, [((B // T, 2 * wide), BF16)] * C, pos, keep, give)
        ends.append(blocks[0])
        for d in range(1, C):
            ends.append(L.along_h(blocks[d], d))
    return kernel(
        last_body, [((B // T, D), BF16)], pos, *ends, scratch=[pltpu.VMEM((16, B // T, rows), F32)]
    )


def solution(mesh):
    in_specs = (
        P("sp", None),
        P(),
        P("sp", "tp"),
        P("sp", "tp"),
        P(None, "tp"),
        P("tp"),
        P("tp"),
        P("sp", "tp"),
        P("sp", "tp"),
        P("sp", "tp"),
        P(),
        P(None, None, "tp", "sp"),
        P(None, "tp", None, None),
        P(None, "tp", None),
        P(None, "tp"),
        P("tp"),
        P("sp", "tp"),
        P("sp", "tp"),
    )
    out_specs = P(("sp", "tp"), None)
    return jax.shard_map(shards, mesh=mesh, in_specs=in_specs, out_specs=out_specs, check_vma=False)
```
